128 devices in a mesh: sp: 16 (over z, x), tp: 8 (over y, core).
Axes of the slice: x: 4, y: 4, z: 4, core: 2. Of those that a mesh axis runs over, the one named last changes fastest.
Arguments:
- tokens: bfloat16 [4, 16384, 2048], P(None, 'sp'), may hold values from -6 to 6
- norm_gain: bfloat16 [2048], replicated, may hold values from 0.099609375 to 1.8984375
- conv_value_weight: bfloat16 [2048, 1024], P('sp', 'tp'), may hold values from -0.125 to 0.125
- conv_gate_weight: bfloat16 [2048, 1024], P('sp', 'tp'), may hold values from -0.125 to 0.125
- query_weight: bfloat16 [2048, 1024], P('sp', 'tp'), may hold values from -40 to 40
- key_weight: bfloat16 [2048, 512], P('sp', 'tp'), may hold values from -1 to 1
- value_weight: bfloat16 [2048, 512], P('sp', 'tp'), may hold values from -0.125 to 0.125
- conv_taps: bfloat16 [31, 1024], P(None, 'tp'), may hold values from -1 to 1
- conv_gain: bfloat16 [1024], P('tp'), may hold values from 0.099609375 to 1.8984375
- sink_logit: float32 [16], P('tp'), may hold values from 1 to 6
- out_conv_weight: bfloat16 [1024, 2048], P('tp', 'sp'), may hold values from -0.125 to 0.125
- out_attn_weight: bfloat16 [1024, 2048], P('tp', 'sp'), may hold values from -0.125 to 0.125
Outputs:
- mixed: bfloat16 [4, 16384, 2048], P(None, ('sp', 'tp'))
- log_total: float32 [4, 16, 16384], P(None, 'tp', 'sp')
The draws below stay inside these ranges and needn't reach their ends.
All inputs are finite; a program needn't handle non-finite values.
Results may differ from the reference program's by a relative error of at most 0.015.
Values may be sent and summed in bfloat16 or wider, within the bound.
No kernel may reach another device: no remote copies, remote signals or barrier semaphores. Data moves between devices by JAX's collectives and lax.ppermute only.
A program may use at most 128 MiB of HBM per device.

```python
import math
import jax
import jax.numpy as jnp
from jax import lax

D = 2048
CONV_CH = 1024
HEADS = 16
KV_HEADS = 8
HEAD_DIM = 64
WINDOW = 128
CONV_K = 31
SEQS = 4
SEQ = 16384


def shared_keys(key):
    drawn = jax.random.truncated_normal(jax.random.fold_in(key, 71), -6.0, 6.0, (D, KV_HEADS * HEAD_DIM), jnp.float32)
    return drawn / jnp.sqrt(jnp.float32(D))


def draw_key_weight(key, part):
    return shared_keys(key).astype(jnp.bfloat16)


def draw_query_weight(key, part):
    drawn = jax.random.truncated_normal(jax.random.fold_in(key, 73), -6.0, 6.0, (D, HEADS * HEAD_DIM), jnp.float32)
    drawn = drawn / jnp.sqrt(jnp.float32(D))
    return drawn.astype(jnp.bfloat16)


def levels(stream_key, shape, split, smallest, largest):
    def one(dim, shards_of):
        heights = jax.random.uniform(jax.random.fold_in(jax.random.fold_in(stream_key, 6), dim), (shards_of,), jnp.float32, smallest / len(split), largest / len(split))
        return jnp.repeat(jnp.exp(heights), shape[dim] // shards_of).reshape((-1,) + (1,) * (len(shape) - dim - 1))

    gain = one(*split[0])
    for cut in split[1:]:
        gain = gain * one(*cut)
    return gain


def noise(key, dims, deviation, limit, pieces=(), kind=jnp.bfloat16):
    loudness = levels(key, dims, pieces, -0.22, 0.18) if pieces else 1.0
    result = jax.random.normal(key, dims, jnp.float32) * deviation * loudness
    return jnp.minimum(jnp.maximum(result, -limit), limit).astype(kind)


def setup_inputs(seed: int = 0) -> dict:
    streams_of = jax.random.split(jax.random.key(seed), 13)
    tokens = noise(streams_of[0], (SEQS, SEQ, D), 1.0, 6.0, ((1, 16),))
    norm_gain = jnp.clip(1.0 + 0.18 * jax.random.normal(streams_of[1], (D,), jnp.float32), 0.099609375, 1.8984375).astype(jnp.bfloat16)
    conv_value_weight = noise(streams_of[2], (D, CONV_CH), D ** -0.5, 0.125, ((0, 16), (1, 8)))
    conv_gate_weight = noise(streams_of[3], (D, CONV_CH), D ** -0.5, 0.125, ((0, 16), (1, 8)))
    query_weight = draw_query_weight(jax.random.fold_in(streams_of[12], 71), 0)
    key_weight = draw_key_weight(jax.random.fold_in(streams_of[12], 71), 0)
    value_weight = noise(streams_of[6], (D, KV_HEADS * HEAD_DIM), D ** -0.5, 0.125, ((0, 16), (1, 8)))
    conv_taps = noise(streams_of[7], (CONV_K, CONV_CH), CONV_K ** -0.5, 1.0, ((1, 8),))
    conv_gain = jnp.clip(1.0 + 0.18 * jax.random.normal(streams_of[8], (CONV_CH,), jnp.float32), 0.099609375, 1.8984375).astype(jnp.bfloat16)
    sink_logit = jnp.clip(1.0 + 5.0 * jax.random.uniform(streams_of[9], (HEADS,), jnp.float32) ** levels(streams_of[9], (HEADS,), ((0, 8),), -0.2, 0.2), 1.0, 6.0)
    out_conv_weight = noise(streams_of[10], (CONV_CH, D), (CONV_CH + HEADS * HEAD_DIM) ** -0.5, 0.125, ((0, 8), (1, 16)))
    out_attn_weight = noise(streams_of[11], (HEADS * HEAD_DIM, D), (CONV_CH + HEADS * HEAD_DIM) ** -0.5, 0.125, ((0, 8), (1, 16)))
    return dict(tokens=tokens, norm_gain=norm_gain, conv_value_weight=conv_value_weight, conv_gate_weight=conv_gate_weight, query_weight=query_weight, key_weight=key_weight, value_weight=value_weight, conv_taps=conv_taps, conv_gain=conv_gain, sink_logit=sink_logit, out_conv_weight=out_conv_weight, out_attn_weight=out_attn_weight)


EPSILON = 1e-06
ROPE_BASE = 10000.0
MASK_VALUE = -1e+30

def rotate(raw, positions):
    half_dim = raw.shape[-1] // 2
    inverse = ROPE_BASE ** (-jnp.arange(half_dim, dtype=jnp.float32) / half_dim)
    angles = positions[:, None] * inverse[None, :]
    cosine = jnp.cos(angles)[None, :, None, :]
    sine = jnp.sin(angles)[None, :, None, :]
    first, second = (raw[..., :half_dim], raw[..., half_dim:])
    return jnp.concatenate([first * cosine - second * sine, first * sine + second * cosine], axis=-1)

def reference(tokens, norm_gain, conv_value_weight, conv_gate_weight, query_weight, key_weight, value_weight, conv_taps, conv_gain, sink_logit, out_conv_weight, out_attn_weight):
    seq_count, seq_len, width = tokens.shape
    floats = tokens.astype(jnp.float32)
    row_mean = floats.mean(-1, keepdims=True)
    centred = floats - row_mean
    variance = lax.optimization_barrier(jnp.mean(centred * centred, -1, keepdims=True))
    normed = (centred * lax.rsqrt(variance + EPSILON) * norm_gain.astype(jnp.float32)).astype(jnp.bfloat16)
    flat = normed.reshape(-1, width)
    conv_value = jnp.dot(flat, conv_value_weight, preferred_element_type=jnp.float32)
    conv_gate = jnp.dot(flat, conv_gate_weight, preferred_element_type=jnp.float32)
    gated = (conv_value * jax.nn.sigmoid(conv_gate)).astype(jnp.bfloat16).reshape(seq_count, seq_len, CONV_CH)
    rim = CONV_K // 2
    padded = jnp.pad(gated, ((0, 0), (rim, rim), (0, 0)))
    taps = conv_taps.astype(jnp.float32)
    filtered = jnp.zeros((seq_count, seq_len, CONV_CH), jnp.float32)
    for tap_index in range(CONV_K):
        filtered = filtered + padded[:, tap_index:tap_index + seq_len].astype(jnp.float32) * taps[tap_index]
    chan_mean = filtered.mean(-1, keepdims=True)
    chan_centred = filtered - chan_mean
    chan_var = lax.optimization_barrier(jnp.mean(chan_centred * chan_centred, -1, keepdims=True))
    conv_out = jax.nn.silu(chan_centred * lax.rsqrt(chan_var + EPSILON) * conv_gain.astype(jnp.float32))
    conv_out = conv_out.astype(jnp.bfloat16)
    group = HEADS // KV_HEADS
    positions = jnp.arange(seq_len, dtype=jnp.float32)
    query_raw = jnp.dot(flat, query_weight, preferred_element_type=jnp.float32)
    key_raw = jnp.dot(flat, key_weight, preferred_element_type=jnp.float32)
    queries = rotate(query_raw.reshape(seq_count, seq_len, HEADS, HEAD_DIM), positions).astype(jnp.bfloat16)
    queries = queries.reshape(seq_count, seq_len, KV_HEADS, group, HEAD_DIM)
    keys = rotate(key_raw.reshape(seq_count, seq_len, KV_HEADS, HEAD_DIM), positions).astype(jnp.bfloat16)
    values = jnp.dot(flat, value_weight, preferred_element_type=jnp.float32).astype(jnp.bfloat16)
    values = values.reshape(seq_count, seq_len, KV_HEADS, HEAD_DIM)
    edge = ((0, 0), (WINDOW, WINDOW), (0, 0), (0, 0))
    keys_pad = jnp.pad(keys, edge)
    values_pad = jnp.pad(values, edge)
    block_rows = math.gcd(seq_len, 512)
    span_len = block_rows + 2 * WINDOW
    score_scale = HEAD_DIM ** (-0.5)
    sink = sink_logit.astype(jnp.float32).reshape(KV_HEADS, group)[None, :, :, None]
    relative = jnp.arange(span_len)[None, :] - jnp.arange(block_rows)[:, None]
    band = (relative >= 0) & (relative <= 2 * WINDOW)

    def one_block(block):
        first_row = (block * block_rows).astype(jnp.int32)
        q_block = lax.dynamic_slice_in_dim(queries, first_row, block_rows, 1).astype(jnp.float32)
        k_block = lax.dynamic_slice_in_dim(keys_pad, first_row, span_len, 1).astype(jnp.float32)
        v_block = lax.dynamic_slice_in_dim(values_pad, first_row, span_len, 1).astype(jnp.float32)
        scores = jnp.einsum('sqkgd,spkd->skgqp', q_block, k_block) * score_scale
        key_pos = first_row - WINDOW + jnp.arange(span_len, dtype=jnp.int32)
        allowed = band & ((key_pos >= 0) & (key_pos < seq_len))[None, :]
        scores = jnp.where(allowed, scores, MASK_VALUE)
        top = jnp.maximum(scores.max(-1), sink)
        weights = jnp.exp(scores - top[..., None])
        total = weights.sum(-1) + jnp.exp(sink - top)
        probs = (weights / total[..., None]).astype(jnp.bfloat16).astype(jnp.float32)
        out = jnp.einsum('skgqp,spkd->sqkgd', probs, v_block).astype(jnp.bfloat16)
        return (out, top + jnp.log(total))
    outs, totals = lax.map(one_block, jnp.arange(seq_len // block_rows, dtype=jnp.int32))
    attn_out = jnp.moveaxis(outs, 0, 1).reshape(seq_count * seq_len, HEADS * HEAD_DIM)
    log_total = jnp.moveaxis(totals, 0, 3).reshape(seq_count, HEADS, seq_len)
    mixed = jnp.dot(conv_out.reshape(-1, CONV_CH), out_conv_weight, preferred_element_type=jnp.float32) + jnp.dot(attn_out, out_attn_weight, preferred_element_type=jnp.float32)
    return (mixed.astype(jnp.bfloat16).reshape(seq_count, seq_len, width), log_total)
```

```python
import functools

import jax
import jax.numpy as jnp
from jax import lax
from jax.experimental import pallas as pl
from jax.experimental.pallas import tpu as pltpu
from jax.sharding import PartitionSpec as P

HEAD_DIM = 64
WINDOW = 128
EPSILON = 1e-06
ROPE_BASE = 10000.0
MASK_VALUE = -1e30
LANES = 128
EDGE = 16
Q_BLOCK = 256
BF16 = jnp.bfloat16
F32 = jnp.float32


def params(*semantics, mb=48):
    return pltpu.CompilerParams(
        dimension_semantics=semantics, vmem_limit_bytes=mb * 1024 * 1024
    )


def norm_kernel(x_ref, gain_ref, out_ref):
    x = x_ref[...].astype(F32)
    mean = jnp.mean(x, axis=-1, keepdims=True)
    centred = x - mean
    variance = jnp.mean(centred * centred, axis=-1, keepdims=True)
    scaled = centred * lax.rsqrt(variance + EPSILON)
    out_ref[...] = (scaled * gain_ref[...].astype(F32)).astype(BF16)


def norm_tokens(x, gain, block=256):
    rows, width = x.shape
    return pl.pallas_call(
        norm_kernel,
        grid=(rows // block,),
        in_specs=[
            pl.BlockSpec((block, width), lambda i: (i, 0)),
            pl.BlockSpec((1, width), lambda i: (0, 0)),
        ],
        out_specs=pl.BlockSpec((block, width), lambda i: (i, 0)),
        out_shape=jax.ShapeDtypeStruct((rows, width), BF16),
        compiler_params=params("arbitrary"),
        cost_estimate=pl.CostEstimate(
            flops=40 * rows * width, transcendentals=rows, bytes_accessed=4 * rows * width
        ),
        name="norm_tokens",
    )(x, gain.reshape(1, width))


def project_kernel(x_ref, w_ref, cos_ref, sin_ref, gated_ref, q_ref, kv_ref):
    pieces, rows, cols = w_ref.shape
    raw = jnp.dot(
        x_ref[...], w_ref[...].reshape(pieces * rows, cols), preferred_element_type=F32
    )
    value, gate = raw[:, :LANES], raw[:, LANES : 2 * LANES]
    gated_ref[...] = (value * jax.nn.sigmoid(gate)).astype(BF16)
    lane = lax.broadcasted_iota(jnp.int32, value.shape, 1)
    low = (lane % HEAD_DIM) < HEAD_DIM // 2
    half = HEAD_DIM // 2
    for part, ref, scale in ((2, q_ref, HEAD_DIM**-0.5), (3, kv_ref, None)):
        x = raw[:, part * LANES : (part + 1) * LANES]
        partner = jnp.where(low, pltpu.roll(x, LANES - half, 1), pltpu.roll(x, half, 1))
        at = slice((part - 2) * LANES, (part - 1) * LANES)
        turned = x * cos_ref[:, at] + partner * sin_ref[:, at]
        if scale is not None:
            turned = turned * scale
        ref[...] = turned.astype(BF16)


def project(normed, weight, cosine, sine, block=512):
    rows, width = normed.shape
    per_seq = cosine.shape[0] // block
    out = pl.BlockSpec((block, LANES), lambda i: (i, 0))
    return pl.pallas_call(
        project_kernel,
        grid=(rows // block,),
        in_specs=[
            pl.BlockSpec((block, width), lambda i: (i, 0)),
            pl.BlockSpec(weight.shape, lambda i: (0, 0, 0)),
            pl.BlockSpec((block, 2 * LANES), lambda i: (i % per_seq, 0)),
            pl.BlockSpec((block, 2 * LANES), lambda i: (i % per_seq, 0)),
        ],
        out_specs=[out, out, out],
        out_shape=[jax.ShapeDtypeStruct((rows, LANES), BF16)] * 3,
        compiler_params=params("arbitrary"),
        cost_estimate=pl.CostEstimate(
            flops=2 * rows * width * weight.shape[2],
            transcendentals=0,
            bytes_accessed=2 * rows * width,
        ),
        name="project",
    )(normed, weight, cosine, sine)


def conv_kernel(before_ref, x_ref, after_ref, taps_ref, out_ref, buf_ref, *, chunk):
    length = x_ref.shape[1]
    buf_ref[0:EDGE, :] = before_ref[0].astype(F32)
    buf_ref[EDGE : EDGE + length, :] = x_ref[0].astype(F32)
    buf_ref[EDGE + length : 2 * EDGE + length, :] = after_ref[0].astype(F32)
    tap_count = taps_ref.shape[0]
    shift = EDGE - tap_count // 2
    dests, _, share, _ = out_ref.shape

    def one(dest, _):
        for part in range(share // chunk):
            total = jnp.zeros((chunk, LANES), F32)
            for tap in range(tap_count):
                at = dest * share + (part * chunk + shift + tap)
                total = total + buf_ref[pl.ds(at, chunk), :] * taps_ref[tap : tap + 1, :]
            out_ref[dest, 0, pl.ds(part * chunk, chunk), :] = total.astype(BF16)
        return 0

    lax.fori_loop(0, dests, one, 0)


def conv(before, gated, after, taps, dests, chunk=64):
    seqs, length, _ = gated.shape
    edge = pl.BlockSpec((1, EDGE, LANES), lambda s: (s, 0, 0))
    return pl.pallas_call(
        functools.partial(conv_kernel, chunk=chunk),
        grid=(seqs,),
        in_specs=[
            edge,
            pl.BlockSpec((1, length, LANES), lambda s: (s, 0, 0)),
            edge,
            pl.BlockSpec(taps.shape, lambda s: (0, 0)),
        ],
        out_specs=pl.BlockSpec((dests, 1, length // dests, LANES), lambda s: (0, s, 0, 0)),
        out_shape=jax.ShapeDtypeStruct((dests, seqs, length // dests, LANES), BF16),
        scratch_shapes=[pltpu.VMEM((length + 2 * EDGE, LANES), F32)],
        compiler_params=params("arbitrary"),
        cost_estimate=pl.CostEstimate(
            flops=60 * 31 * seqs * length * LANES,
            transcendentals=0,
            bytes_accessed=4 * seqs * length * LANES,
        ),
        name="conv",
    )(before, gated, after, taps)


def attend_kernel(
    place_ref, sink_ref, q_ref, before_ref, kv_ref, after_ref, out_ref, log_ref, pad_ref, bias_ref
):
    length = kv_ref.shape[1]
    seq, block = pl.program_id(0), pl.program_id(1)
    blocks = length // Q_BLOCK
    span = Q_BLOCK + 2 * WINDOW

    @pl.when((seq == 0) & (block == 0))
    def _():
        query = lax.broadcasted_iota(jnp.int32, (Q_BLOCK, span), 0)
        key = lax.broadcasted_iota(jnp.int32, (Q_BLOCK, span), 1)
        band = (key >= query) & (key <= query + 2 * WINDOW)
        first = jnp.where(place_ref[0] == 0, WINDOW, 0)
        last = jnp.where(place_ref[0] == place_ref[1] - 1, Q_BLOCK + WINDOW, span)
        zero, out = jnp.zeros(band.shape, F32), jnp.full(band.shape, MASK_VALUE, F32)
        bias_ref[0] = jnp.where(band, zero, out)
        bias_ref[1] = jnp.where(band & (key >= first), zero, out)
        bias_ref[2] = jnp.where(band & (key < last), zero, out)

    @pl.when(block == 0)
    def _():
        pad_ref[0:WINDOW, :] = before_ref[0]
        pad_ref[WINDOW : WINDOW + length, :] = kv_ref[0]
        pad_ref[WINDOW + length : 2 * WINDOW + length, :] = after_ref[0]

    keys = pad_ref[pl.ds(pl.multiple_of(block * Q_BLOCK, Q_BLOCK), span), :]
    bias = bias_ref[jnp.where(block == 0, 1, jnp.where(block == blocks - 1, 2, 0))]
    query = q_ref[0].astype(F32)
    lane = lax.broadcasted_iota(jnp.int32, (Q_BLOCK, LANES), 1)
    low = lane < HEAD_DIM
    sub = lax.broadcasted_iota(jnp.int32, (LANES, LANES), 0)
    diagonal = sub == lax.broadcasted_iota(jnp.int32, (LANES, LANES), 1)
    results = []
    for head in range(2):
        turned = query if head == 0 else pltpu.roll(query, HEAD_DIM, 1)
        own = jnp.where(low, turned, 0.0).astype(BF16)
        scores = lax.dot_general(
            own, keys, (((1,), (1,)), ((), ())), preferred_element_type=F32
        )
        scores = scores + bias
        sink = sink_ref[head]
        top = jnp.maximum(jnp.max(scores, axis=-1, keepdims=True), sink)
        weights = jnp.exp(scores - top)
        total = jnp.sum(weights, axis=-1, keepdims=True) + jnp.exp(sink - top)
        mixed = jnp.dot(weights.astype(BF16), keys, preferred_element_type=F32)
        results.append(mixed / total)
        log_total = jnp.broadcast_to(top + jnp.log(total), (Q_BLOCK, LANES))
        for part in range(Q_BLOCK // LANES):
            rows = log_total[part * LANES : (part + 1) * LANES]
            log_ref[0, head : head + 1, part * LANES : (part + 1) * LANES] = jnp.sum(
                jnp.where(diagonal, rows, 0.0), axis=0, keepdims=True
            )
    both = jnp.where(low, pltpu.roll(results[0], HEAD_DIM, 1), results[1]).astype(BF16)
    share = out_ref.shape[2]
    out_ref[...] = both.reshape(Q_BLOCK // share, 1, share, LANES)


def attend(place, sink, query, before, kv, after, dests):
    seqs, length, _ = kv.shape
    share = length // dests
    span = Q_BLOCK + 2 * WINDOW
    edge = pl.BlockSpec((1, WINDOW, LANES), lambda s, b: (s, 0, 0))
    smem = pl.BlockSpec(memory_space=pltpu.SMEM)
    return pl.pallas_call(
        attend_kernel,
        grid=(seqs, length // Q_BLOCK),
        in_specs=[
            smem,
            smem,
            pl.BlockSpec((1, Q_BLOCK, LANES), lambda s, b: (s, b, 0)),
            edge,
            pl.BlockSpec((1, length, LANES), lambda s, b: (s, 0, 0)),
            edge,
        ],
        out_specs=[
            pl.BlockSpec((Q_BLOCK // share, 1, share, LANES), lambda s, b: (b, s, 0, 0)),
            pl.BlockSpec((1, 2, Q_BLOCK), lambda s, b: (s, 0, b)),
        ],
        out_shape=[
            jax.ShapeDtypeStruct((dests, seqs, share, LANES), BF16),
            jax.ShapeDtypeStruct((seqs, 2, length), F32),
        ],
        scratch_shapes=[
            pltpu.VMEM((length + 2 * WINDOW, LANES), BF16),
            pltpu.VMEM((3, Q_BLOCK, span), F32),
        ],
        compiler_params=params("arbitrary", "arbitrary"),
        cost_estimate=pl.CostEstimate(
            flops=40 * seqs * length * span * LANES // 8,
            transcendentals=0,
            bytes_accessed=6 * seqs * length * LANES,
        ),
        name="attend",
    )(place, sink, query, before, kv, after)


def mix_kernel(conv_ref, attn_ref, gain_ref, w_ref, out_ref, act_ref):
    sources = conv_ref.shape[0]
    half = sources * LANES

    @pl.when(pl.program_id(0) == 0)
    def _():
        x = jnp.concatenate([conv_ref[s] for s in range(sources)], axis=-1).astype(F32)
        mean = jnp.mean(x, axis=-1, keepdims=True)
        centred = x - mean
        variance = jnp.mean(centred * centred, axis=-1, keepdims=True)
        v = centred * lax.rsqrt(variance + EPSILON) * gain_ref[...].astype(F32)
        act_ref[:, :half] = (v / (1.0 + jnp.exp(-v))).astype(BF16)
        for s in range(sources):
            act_ref[:, half + s * LANES : half + (s + 1) * LANES] = attn_ref[s]

    cols = w_ref.shape[0]
    conv_w = jnp.concatenate([w_ref[c, :, :LANES].reshape(half, LANES) for c in range(cols)], -1)
    attn_w = jnp.concatenate(
        [w_ref[c, :, LANES : 2 * LANES].reshape(half, LANES) for c in range(cols)], -1
    )
    total = jnp.dot(act_ref[:, :half], conv_w, preferred_element_type=F32)
    total = total + jnp.dot(act_ref[:, half:], attn_w, preferred_element_type=F32)
    out_ref[...] = total.astype(BF16)


def mix(conv_tok, attn_tok, gain, weight, cols=2):
    sources, rows, _ = conv_tok.shape
    groups, _, height, _ = weight.shape
    whole = pl.BlockSpec((sources, rows, LANES), lambda n: (0, 0, 0))
    return pl.pallas_call(
        mix_kernel,
        grid=(groups // cols,),
        in_specs=[
            whole,
            whole,
            pl.BlockSpec(gain.shape, lambda n: (0, 0)),
            pl.BlockSpec((cols, sources, height, LANES), lambda n: (n, 0, 0, 0)),
        ],
        out_specs=pl.BlockSpec((rows, cols * LANES), lambda n: (0, n)),
        out_shape=jax.ShapeDtypeStruct((rows, groups * LANES), BF16),
        scratch_shapes=[pltpu.VMEM((rows, 2 * sources * LANES), BF16)],
        compiler_params=params("arbitrary"),
        cost_estimate=pl.CostEstimate(
            flops=4 * rows * sources * LANES * groups * LANES,
            transcendentals=0,
            bytes_accessed=2 * weight.size,
        ),
        name="mix",
    )(conv_tok, attn_tok, gain, weight)


def turn_tables(tok_count):
    half = HEAD_DIM // 2
    offset = lax.axis_index("sp") * tok_count
    positions = (offset + jnp.arange(tok_count, dtype=jnp.int32)).astype(F32)
    inverse = ROPE_BASE ** (-jnp.arange(half, dtype=F32) / half)
    angles = positions[:, None] * inverse[None, :]
    c, s = jnp.cos(angles), jnp.sin(angles)
    one, zero = jnp.ones_like(c), jnp.zeros_like(s)
    cosine = jnp.concatenate([c, c, c, c, c, c, one, one], axis=-1)
    sine = jnp.concatenate([-s, s, -s, s, -s, s, zero, zero], axis=-1)
    return cosine, sine


def on_device(
    tokens,
    norm_gain,
    conv_value_weight,
    conv_gate_weight,
    query_weight,
    key_weight,
    value_weight,
    conv_taps,
    conv_gain,
    sink_logit,
    out_conv_weight,
    out_attn_weight,
):
    seqs, length, width = tokens.shape
    sp, tp = lax.axis_size("sp"), lax.axis_size("tp")
    place = jnp.stack([lax.axis_index("sp"), jnp.int32(sp)]).astype(jnp.int32)

    gain_rows = jnp.broadcast_to(conv_gain[None], (EDGE, LANES))
    out_piece = jnp.concatenate([out_conv_weight, out_attn_weight, gain_rows], axis=0)
    out_weight = lax.all_gather(out_piece, ("sp", "tp"), axis=0, tiled=True)
    out_weight = out_weight.reshape(sp, tp, out_piece.shape[0], LANES)

    in_piece = jnp.concatenate(
        [conv_value_weight, conv_gate_weight, query_weight, key_weight, value_weight], axis=1
    )
    in_weight = lax.all_to_all(
        jnp.broadcast_to(in_piece[None], (sp, *in_piece.shape)), "sp", 0, 0, tiled=True
    )
    normed = norm_tokens(tokens.reshape(seqs * length, width), norm_gain)
    cosine, sine = turn_tables(length)
    gated, query, kv = (
        a.reshape(seqs, length, LANES) for a in project(normed, in_weight, cosine, sine)
    )

    up = [(i, i + 1) for i in range(sp - 1)]
    down = [(i + 1, i) for i in range(sp - 1)]
    low = jnp.concatenate([kv[:, :WINDOW], gated[:, :EDGE]], axis=1)
    high = jnp.concatenate([kv[:, -WINDOW:], gated[:, -EDGE:]], axis=1)
    before = lax.ppermute(high, "sp", up)
    after = lax.ppermute(low, "sp", down)

    filtered = conv(
        before[:, WINDOW:], gated, after[:, WINDOW:], conv_taps.astype(F32), tp
    )
    conv_tok = lax.all_to_all(filtered, "tp", 0, 0, tiled=True)
    attn, log_total = attend(
        place, sink_logit, query, before[:, :WINDOW], kv, after[:, :WINDOW], tp
    )
    attn_tok = lax.all_to_all(attn, "tp", 0, 0, tiled=True)

    gain = out_weight[0, :, 2 * LANES].reshape(1, tp * LANES)
    rows = seqs * length // tp
    mixed = mix(
        conv_tok.reshape(tp, rows, LANES), attn_tok.reshape(tp, rows, LANES), gain, out_weight
    )
    return mixed.reshape(seqs, length // tp, width), log_total


def solution(mesh):
    placed = (
        P(None, "sp", None),
        P(),
        P("sp", "tp"),
        P("sp", "tp"),
        P("sp", "tp"),
        P("sp", "tp"),
        P("sp", "tp"),
        P(None, "tp"),
        P("tp"),
        P("tp"),
        P("tp", "sp"),
        P("tp", "sp"),
    )
    return jax.shard_map(
        on_device,
        mesh=mesh,
        in_specs=placed,
        out_specs=(P(None, ("sp", "tp"), None), P(None, "tp", "sp")),
        check_vma=False,
    )
```

```python
import functools

import jax
import jax.numpy as jnp
from jax import lax
from jax.experimental import pallas as pl
from jax.experimental.pallas import tpu as pltpu
from jax.sharding import PartitionSpec as P

HEAD_DIM = 64
WINDOW = 128
EPSILON = 1e-06
ROPE_BASE = 10000.0
MASK_VALUE = -1e30
LANES = 128
EDGE = 16
Q_BLOCK = 128
BF16 = jnp.bfloat16
F32 = jnp.float32


def in_hbm(value):
    return pltpu.with_memory_space_constraint(value, pltpu.HBM)


def params(*semantics, mb=48):
    return pltpu.CompilerParams(
        dimension_semantics=semantics, vmem_limit_bytes=mb * 1024 * 1024
    )


def norm_kernel(x_ref, gain_ref, out_ref):
    x = x_ref[...].astype(F32)
    mean = jnp.mean(x, axis=-1, keepdims=True)
    centred = x - mean
    variance = jnp.mean(centred * centred, axis=-1, keepdims=True)
    scaled = centred * lax.rsqrt(variance + EPSILON) * gain_ref[...].astype(F32)
    out_ref[...] = scaled.astype(BF16)


def norm_tokens(x, gain, block=512):
    rows, width = x.shape
    block = min(block, rows)
    return pl.pallas_call(
        norm_kernel,
        grid=(rows // block,),
        in_specs=[
            pl.BlockSpec((block, width), lambda i: (i, 0)),
            pl.BlockSpec((1, width), lambda i: (0, 0)),
        ],
        out_specs=pl.BlockSpec((block, width), lambda i: (i, 0)),
        out_shape=pltpu.HBM((rows, width), BF16),
        compiler_params=params("arbitrary", mb=28),
        cost_estimate=pl.CostEstimate(
            flops=40 * rows * width, transcendentals=rows, bytes_accessed=4 * rows * width
        ),
        name="norm_tokens",
    )(in_hbm(x), gain.reshape(1, width))


def project_kernel(
    x_ref, edge_ref, w_ref, taps_ref, cos_ref, sin_ref, out_ref, q_ref, kv_ref, buf_ref, *, sub, chunk
):
    step = pl.program_id(0)
    dests, _, share, _ = out_ref.shape
    length, seqs = dests * share, edge_ref.shape[0]
    half = HEAD_DIM // 2
    tap_count = taps_ref.shape[0]
    shift = EDGE - tap_count // 2
    slot, last = step % 2, (step + 1) % 2

    def gate(raw):
        return raw[:, :LANES] * jax.nn.sigmoid(raw[:, LANES : 2 * LANES])

    def filter_rows(first):
        for at in range(first, first + sub, chunk):
            total = jnp.zeros((chunk, LANES), F32)
            for tap in range(tap_count):
                rows = buf_ref[last, at + shift + tap : at + shift + tap + chunk, :]
                total = total + rows * taps_ref[tap : tap + 1, :]
            out_ref[at // share, 0, at % share : at % share + chunk, :] = total.astype(BF16)

    @pl.when(step < seqs)
    def _():
        weight = w_ref[...].reshape(-1, w_ref.shape[2])
        low = (lax.broadcasted_iota(jnp.int32, (sub, LANES), 1) % HEAD_DIM) < half
        ends = gate(
            jnp.dot(edge_ref[step], weight[:, : 2 * LANES], preferred_element_type=F32)
        ).astype(BF16).astype(F32)
        buf_ref[slot, 0:EDGE, :] = ends[:EDGE]
        buf_ref[slot, EDGE + length : 2 * EDGE + length, :] = ends[EDGE:]
        for first in range(0, length, sub):
            raw = jnp.dot(x_ref[first : first + sub, :], weight, preferred_element_type=F32)
            filter_rows(first)
            buf_ref[slot, EDGE + first : EDGE + first + sub, :] = (
                gate(raw).astype(BF16).astype(F32)
            )
            table = slice(first, first + sub)
            for part, ref, scale in ((2, q_ref, HEAD_DIM**-0.5), (3, kv_ref, None)):
                x = raw[:, part * LANES : (part + 1) * LANES]
                partner = jnp.where(low, pltpu.roll(x, LANES - half, 1), pltpu.roll(x, half, 1))
                at = slice((part - 2) * LANES, (part - 1) * LANES)
                turned = x * cos_ref[table, at] + partner * sin_ref[table, at]
                if scale is not None:
                    turned = turned * scale
                ref[0, table, :] = turned.astype(BF16)

    @pl.when(step == seqs)
    def _():
        for first in range(0, length, sub):
            filter_rows(first)


def project(normed, edges, weight, taps, cosine, sine, dests, sub=256, chunk=32):
    seqs = edges.shape[0]
    rows, width = normed.shape
    length = rows // seqs
    inside = pl.BlockSpec(memory_space=pltpu.VMEM)
    heads = pltpu.HBM((seqs, length, LANES), BF16)
    head_block = pl.BlockSpec((1, length, LANES), lambda s: (jnp.minimum(s, seqs - 1), 0, 0))
    return pl.pallas_call(
        functools.partial(project_kernel, sub=sub, chunk=chunk),
        grid=(seqs + 1,),
        in_specs=[pl.BlockSpec((length, width), lambda s: (jnp.minimum(s, seqs - 1), 0))]
        + [inside] * 5,
        out_specs=[
            pl.BlockSpec(
                (dests, 1, length // dests, LANES), lambda s: (0, jnp.maximum(s - 1, 0), 0, 0)
            ),
            head_block,
            head_block,
        ],
        out_shape=[
            jax.ShapeDtypeStruct((dests, seqs, length // dests, LANES), BF16), heads, heads
        ],
        scratch_shapes=[pltpu.VMEM((2, length + 2 * EDGE, LANES), F32)],
        compiler_params=params("arbitrary", mb=28),
        cost_estimate=pl.CostEstimate(
            flops=2 * rows * width * weight.shape[2],
            transcendentals=0,
            bytes_accessed=2 * rows * width,
        ),
        name="project",
    )(in_hbm(normed), edges, weight, taps, cosine, sine)


def attend_kernel(
    place_ref, sink_ref, q_ref, before_ref, kv_ref, after_ref, out_ref, log_ref,
    pad_ref, one_ref, bias_ref,
):
    length = kv_ref.shape[1]
    blocks = length // Q_BLOCK
    span = Q_BLOCK + 2 * WINDOW

    @pl.when(pl.program_id(0) == 0)
    def _():
        query = lax.broadcasted_iota(jnp.int32, (Q_BLOCK, span), 0)
        key = lax.broadcasted_iota(jnp.int32, (Q_BLOCK, span), 1)
        band = (key >= query) & (key <= query + 2 * WINDOW)
        first = jnp.where(place_ref[0] == 0, WINDOW, 0)
        last = jnp.where(place_ref[0] == place_ref[1] - 1, Q_BLOCK + WINDOW, span)
        zero, out = jnp.zeros(band.shape, F32), jnp.full(band.shape, MASK_VALUE, F32)
        bias_ref[0] = jnp.where(band, zero, out)
        bias_ref[1] = jnp.where(band & (key >= first), zero, out)
        bias_ref[2] = jnp.where(band & (key < last), zero, out)

    pad_ref[0:WINDOW, :] = before_ref[0]
    pad_ref[WINDOW : WINDOW + length, :] = kv_ref[0]
    pad_ref[WINDOW + length : 2 * WINDOW + length, :] = after_ref[0]
    padded = pad_ref[...]
    in_low = lax.broadcasted_iota(jnp.int32, padded.shape, 1) < HEAD_DIM
    one_ref[...] = jnp.where(in_low, jnp.ones_like(padded), padded)

    low = lax.broadcasted_iota(jnp.int32, (Q_BLOCK, LANES), 1) < HEAD_DIM
    low_both = lax.broadcasted_iota(jnp.int32, (2 * Q_BLOCK, LANES), 1) < HEAD_DIM
    diagonal = lax.broadcasted_iota(jnp.int32, (LANES, LANES), 0) == lax.broadcasted_iota(
        jnp.int32, (LANES, LANES), 1
    )
    is_first = lax.broadcasted_iota(jnp.int32, (2 * Q_BLOCK, 1), 0) < Q_BLOCK
    sink = jnp.where(is_first, sink_ref[0], sink_ref[1])

    def score(block):
        at = block * Q_BLOCK
        keys = pad_ref[at : at + span, :]
        bias = bias_ref[1 if block == 0 else 2 if block == blocks - 1 else 0]
        query = q_ref[0, at : at + Q_BLOCK, :]
        swapped = pltpu.roll(query.astype(F32), HEAD_DIM, 1).astype(BF16)
        own = jnp.concatenate([query, swapped], 0)
        own = jnp.where(low_both, own, jnp.zeros_like(own))
        scores = lax.dot_general(
            own, keys, (((1,), (1,)), ((), ())), preferred_element_type=F32
        )
        return scores + jnp.concatenate([bias, bias], 0)

    def weigh(block, scores):
        top = jnp.maximum(jnp.max(scores, axis=-1, keepdims=True), sink)
        return top, jnp.exp(scores - top).astype(BF16)

    def blend(block, top, weights):
        at = block * Q_BLOCK
        both = jnp.dot(weights, one_ref[at : at + span, :], preferred_element_type=F32)
        swapped = pltpu.roll(both, HEAD_DIM, 1)
        total = jnp.where(low_both, both, swapped) + jnp.exp(sink - top)
        log_total = top + jnp.log(total)
        for head in range(2):
            log_ref[0, head : head + 1, at : at + Q_BLOCK] = jnp.sum(
                jnp.where(diagonal, log_total[head * Q_BLOCK : (head + 1) * Q_BLOCK], 0.0),
                axis=0,
                keepdims=True,
            )
        first = swapped[:Q_BLOCK] / total[:Q_BLOCK]
        second = both[Q_BLOCK:] / total[Q_BLOCK:]
        out_ref[block, 0] = jnp.where(low, first, second).astype(BF16)

    ahead, behind = score(0), None
    for block in range(blocks):
        scores = ahead
        if block + 1 < blocks:
            ahead = score(block + 1)
        top, weights = weigh(block, scores)
        if behind is not None:
            blend(block - 1, *behind)
        behind = top, weights
    blend(blocks - 1, *behind)


def attend(place, sink, query, before, kv, after, dests):
    seqs, length, _ = kv.shape
    span = Q_BLOCK + 2 * WINDOW
    edge = pl.BlockSpec((1, WINDOW, LANES), lambda s: (s, 0, 0))
    whole = pl.BlockSpec((1, length, LANES), lambda s: (s, 0, 0))
    smem = pl.BlockSpec(memory_space=pltpu.SMEM)
    return pl.pallas_call(
        attend_kernel,
        grid=(seqs,),
        in_specs=[smem, smem, whole, edge, whole, edge],
        out_specs=[
            pl.BlockSpec((dests, 1, length // dests, LANES), lambda s: (0, s, 0, 0)),
            pl.BlockSpec((1, 2, length), lambda s: (s, 0, 0)),
        ],
        out_shape=[
            jax.ShapeDtypeStruct((dests, seqs, length // dests, LANES), BF16),
            jax.ShapeDtypeStruct((seqs, 2, length), F32),
        ],
        scratch_shapes=[
            pltpu.VMEM((length + 2 * WINDOW, LANES), BF16),
            pltpu.VMEM((length + 2 * WINDOW, LANES), BF16),
            pltpu.VMEM((3, Q_BLOCK, span), F32),
        ],
        compiler_params=params("arbitrary"),
        cost_estimate=pl.CostEstimate(
            flops=40 * seqs * length * span * LANES // 8,
            transcendentals=0,
            bytes_accessed=6 * seqs * length * LANES,
        ),
        name="attend",
    )(place, sink, in_hbm(query), before, in_hbm(kv), after)


def side_by_side(ref):
    return jnp.concatenate([ref[i] for i in range(ref.shape[0])], axis=-1)


def columns(ref):
    return jnp.concatenate([ref[c].reshape(-1, LANES) for c in range(ref.shape[0])], axis=-1)


def mix_conv_kernel(x_ref, gain_ref, w_ref, out_ref, act_ref):
    @pl.when(pl.program_id(0) == 0)
    def _():
        x = side_by_side(x_ref).astype(F32)
        gain = side_by_side(gain_ref)[0:1].astype(F32)
        mean = jnp.mean(x, axis=-1, keepdims=True)
        centred = x - mean
        variance = jnp.mean(centred * centred, axis=-1, keepdims=True)
        v = centred * lax.rsqrt(variance + EPSILON) * gain
        act_ref[...] = (v / (1.0 + jnp.exp(-v))).astype(BF16)

    out_ref[...] = jnp.dot(act_ref[...], columns(w_ref), preferred_element_type=F32)


def mix_attn_kernel(x_ref, part_ref, w_ref, out_ref):
    total = part_ref[...] + jnp.dot(
        side_by_side(x_ref), columns(w_ref), preferred_element_type=F32
    )
    out_ref[...] = total.astype(BF16)


def mix(kernel, x, extra, weight, which, out_dtype, cols, name, scratch=()):
    sources, rows, _ = x.shape
    groups = weight.shape[0]
    block = pl.BlockSpec((rows, cols * LANES), lambda n: (0, n))
    if which == 0:
        place = weight.shape[2] // EDGE - 1
        extra_spec = pl.BlockSpec((None, sources, EDGE, LANES), lambda n: (0, 0, place, 0))
    else:
        extra_spec = block
    return pl.pallas_call(
        kernel,
        grid=(groups // cols,),
        in_specs=[
            pl.BlockSpec(x.shape, lambda n: (0, 0, 0)),
            extra_spec,
            pl.BlockSpec((cols, sources, LANES, LANES), lambda n: (n, 0, which, 0)),
        ],
        out_specs=block,
        out_shape=pltpu.HBM((rows, groups * LANES), out_dtype),
        scratch_shapes=list(scratch),
        compiler_params=params("arbitrary", mb=32),
        cost_estimate=pl.CostEstimate(
            flops=2 * rows * sources * LANES * groups * LANES,
            transcendentals=0,
            bytes_accessed=weight.size,
        ),
        name=name,
    )(x, extra, weight)


def pack_kernel(
    value_ref, gate_ref, query_ref, key_ref, kv_ref, conv_ref, attn_ref, gain_ref, out_ref, in_ref
):
    out_ref[0:LANES, :] = conv_ref[...]
    out_ref[LANES : 2 * LANES, :] = attn_ref[...]
    out_ref[2 * LANES :, :] = jnp.broadcast_to(gain_ref[...].astype(F32), (EDGE, LANES)).astype(BF16)
    both = jnp.concatenate([key_ref[...], kv_ref[...]], 0).astype(F32).T.astype(BF16)
    piece = jnp.concatenate([value_ref[...], gate_ref[...], query_ref[...], both], axis=1)
    for copy in range(in_ref.shape[0]):
        in_ref[copy] = piece


def pack(value, gate, query, key, kv, conv, attn, gain, copies):
    rows = value.shape[0]
    cols = 3 * LANES + 2 * key.shape[1]
    return pl.pallas_call(
        pack_kernel,
        out_shape=[
            jax.ShapeDtypeStruct((2 * LANES + EDGE, LANES), BF16),
            jax.ShapeDtypeStruct((copies, rows, cols), BF16),
        ],
        compiler_params=pltpu.CompilerParams(vmem_limit_bytes=16 * 1024 * 1024),
        name="pack",
    )(value, gate, query, key.T, kv.T, conv, attn, gain.reshape(1, LANES))


def turn_tables(tok_count):
    half = HEAD_DIM // 2
    offset = lax.axis_index("sp") * tok_count
    positions = (offset + jnp.arange(tok_count, dtype=jnp.int32)).astype(F32)
    lane = jnp.arange(2 * LANES, dtype=jnp.int32)
    inverse = ROPE_BASE ** (-(lane % half).astype(F32) / half)
    angles = positions[:, None] * inverse[None, :]
    turns = (lane < LANES + HEAD_DIM)[None, :]
    sign = jnp.where(lane % HEAD_DIM < half, -1.0, 1.0).astype(F32)[None, :]
    return jnp.where(turns, jnp.cos(angles), 1.0), jnp.where(turns, jnp.sin(angles) * sign, 0.0)


def on_device(
    tokens,
    norm_gain,
    conv_value_weight,
    conv_gate_weight,
    query_weight,
    key_weight,
    value_weight,
    conv_taps,
    conv_gain,
    sink_logit,
    out_conv_weight,
    out_attn_weight,
):
    seqs, length, width = tokens.shape
    sp, tp = lax.axis_size("sp"), lax.axis_size("tp")
    place = jnp.stack([lax.axis_index("sp"), jnp.int32(sp)]).astype(jnp.int32)
    up = [(i, i + 1) for i in range(sp - 1)]
    down = [(i + 1, i) for i in range(sp - 1)]

    out_piece, in_piece = pack(
        conv_value_weight, conv_gate_weight, query_weight, key_weight, value_weight,
        out_conv_weight, out_attn_weight, conv_gain, sp,
    )
    out_weight = lax.all_gather(out_piece, ("sp", "tp"), axis=0, tiled=True)
    out_weight = out_weight.reshape(sp, tp, out_piece.shape[0], LANES)
    in_weight = lax.all_to_all(in_piece, "sp", 0, 0, tiled=True)

    before = lax.ppermute(tokens[:, -EDGE:], "sp", up)
    after = lax.ppermute(tokens[:, :EDGE], "sp", down)
    normed = norm_tokens(tokens.reshape(seqs * length, width), norm_gain)
    edges = norm_tokens(
        jnp.concatenate([before, after], axis=1).reshape(2 * seqs * EDGE, width), norm_gain
    ).reshape(seqs, 2 * EDGE, width)
    cosine, sine = turn_tables(length)
    filtered, query, kv = project(
        normed, edges, in_weight, conv_taps.astype(F32), cosine, sine, tp
    )

    before = lax.ppermute(kv[:, -WINDOW:], "sp", up)
    after = lax.ppermute(kv[:, :WINDOW], "sp", down)
    conv_tok = lax.all_to_all(filtered, "tp", 0, 0, tiled=True)
    attn, log_total = attend(place, sink_logit, query, before, kv, after, tp)
    attn_tok = lax.all_to_all(attn, "tp", 0, 0, tiled=True)

    rows = seqs * length // tp
    out_weight = in_hbm(out_weight)
    part = mix(
        mix_conv_kernel, conv_tok.reshape(tp, rows, LANES), out_weight, out_weight, 0, F32, 4,
        "mix_conv", [pltpu.VMEM((rows, tp * LANES), BF16)],
    )
    mixed = mix(
        mix_attn_kernel, attn_tok.reshape(tp, rows, LANES), in_hbm(part), out_weight, 1, BF16, 8, "mix_attn"
    )
    return mixed.reshape(seqs, length // tp, width), log_total


def solution(mesh):
    placed = (
        P(None, "sp", None),
        P(),
        P("sp", "tp"),
        P("sp", "tp"),
        P("sp", "tp"),
        P("sp", "tp"),
        P("sp", "tp"),
        P(None, "tp"),
        P("tp"),
        P("tp"),
        P("tp", "sp"),
        P("tp", "sp"),
    )
    return jax.shard_map(
        on_device,
        mesh=mesh,
        in_specs=placed,
        out_specs=(P(None, ("sp", "tp"), None), P(None, "tp", "sp")),
        check_vma=False,
    )
```

```python
import functools

import jax
import jax.numpy as jnp
from jax import lax
from jax.experimental import pallas as pl
from jax.experimental.pallas import tpu as pltpu
from jax.sharding import PartitionSpec as P

HEAD_DIM = 64
WINDOW = 128
EPSILON = 1e-06
ROPE_BASE = 10000.0
MASK_VALUE = -1e30
LANES = 128
EDGE = 16
Q_BLOCK = 128
SPAN = Q_BLOCK + 2 * WINDOW
BF16 = jnp.bfloat16
F32 = jnp.float32


def in_hbm(value):
    return pltpu.with_memory_space_constraint(value, pltpu.HBM)


def params(*semantics, mb=48):
    return pltpu.CompilerParams(
        dimension_semantics=semantics, vmem_limit_bytes=mb * 1024 * 1024
    )


def normalize(x, gain):
    x = x.astype(F32)
    mean = jnp.mean(x, axis=-1, keepdims=True)
    centred = x - mean
    variance = jnp.mean(centred * centred, axis=-1, keepdims=True)
    return centred * lax.rsqrt(variance + EPSILON) * gain.astype(F32)


def norm_kernel(x_ref, gain_ref, out_ref):
    out_ref[...] = normalize(x_ref[...], gain_ref[...]).astype(BF16)


def norm_tokens(x, gain, block=512):
    rows, width = x.shape
    block = min(block, rows)
    return pl.pallas_call(
        norm_kernel,
        grid=(rows // block,),
        in_specs=[
            pl.BlockSpec((block, width), lambda i: (i, 0)),
            pl.BlockSpec((1, width), lambda i: (0, 0)),
        ],
        out_specs=pl.BlockSpec((block, width), lambda i: (i, 0)),
        out_shape=pltpu.HBM((rows, width), BF16),
        compiler_params=params("arbitrary", mb=28),
        cost_estimate=pl.CostEstimate(
            flops=40 * rows * width, transcendentals=rows, bytes_accessed=4 * rows * width
        ),
        name="norm_tokens",
    )(in_hbm(x), gain.reshape(1, width))


def project_kernel(
    x_ref, before_ref, after_ref, gain_ref, w_ref, taps_ref, cos_ref, sin_ref, out_ref, q_ref, kv_ref, buf_ref, *, sub, chunk
):
    step = pl.program_id(0)
    dests, _, share, _ = out_ref.shape
    length, seqs = dests * share, before_ref.shape[0]
    half = HEAD_DIM // 2
    tap_count = taps_ref.shape[0]
    shift = EDGE - tap_count // 2
    slot, last = step % 2, (step + 1) % 2
    taps = taps_ref[...].astype(F32)

    def gate(raw):
        return raw[:, :LANES] * jax.nn.sigmoid(raw[:, LANES : 2 * LANES])

    def filter_rows(first):
        for at in range(first, first + sub, chunk):
            total = jnp.zeros((chunk, LANES), F32)
            for tap in range(tap_count):
                rows = buf_ref[last, at + shift + tap : at + shift + tap + chunk, :]
                total = total + rows * taps[tap : tap + 1, :]
            out_ref[at // share, 0, at % share : at % share + chunk, :] = total.astype(BF16)

    @pl.when(step < seqs)
    def _():
        weight = w_ref[...].reshape(-1, w_ref.shape[2])
        lane = lax.broadcasted_iota(jnp.int32, (sub, LANES), 1)
        low, keyed = (lane % HEAD_DIM) < half, lane < HEAD_DIM
        edges = jnp.concatenate([before_ref[step], after_ref[step]], axis=0)
        edges = normalize(edges, gain_ref[...]).astype(BF16)
        ends = gate(
            jnp.dot(edges, weight[:, : 2 * LANES], preferred_element_type=F32)
        ).astype(BF16).astype(F32)
        buf_ref[slot, 0:EDGE, :] = ends[:EDGE]
        buf_ref[slot, EDGE + length : 2 * EDGE + length, :] = ends[EDGE:]
        for first in range(0, length, sub):
            raw = jnp.dot(x_ref[first : first + sub, :], weight, preferred_element_type=F32)
            filter_rows(first)
            buf_ref[slot, EDGE + first : EDGE + first + sub, :] = (
                gate(raw).astype(BF16).astype(F32)
            )
            table = slice(first, first + sub)
            for part, ref, scale in ((2, q_ref, HEAD_DIM**-0.5), (3, kv_ref, None)):
                x = raw[:, part * LANES : (part + 1) * LANES]
                partner = jnp.where(low, pltpu.roll(x, LANES - half, 1), pltpu.roll(x, half, 1))
                cosine, sine = cos_ref[table, :], sin_ref[table, :]
                if part == 3:
                    cosine, sine = jnp.where(keyed, cosine, 1.0), jnp.where(keyed, sine, 0.0)
                turned = x * cosine + partner * sine
                if scale is not None:
                    turned = turned * scale
                ref[0, table, :] = turned.astype(BF16)

    @pl.when(step == seqs)
    def _():
        for first in range(0, length, sub):
            filter_rows(first)


def project(normed, before, after, gain, weight, taps, cosine, sine, dests, sub=256, chunk=32):
    seqs = before.shape[0]
    rows, width = normed.shape
    length = rows // seqs
    inside = pl.BlockSpec(memory_space=pltpu.VMEM)
    heads = pltpu.HBM((seqs, length, LANES), BF16)
    head_block = pl.BlockSpec((1, length, LANES), lambda s: (jnp.minimum(s, seqs - 1), 0, 0))
    return pl.pallas_call(
        functools.partial(project_kernel, sub=sub, chunk=chunk),
        grid=(seqs + 1,),
        in_specs=[pl.BlockSpec((length, width), lambda s: (jnp.minimum(s, seqs - 1), 0))]
        + [inside] * 7,
        out_specs=[
            pl.BlockSpec(
                (dests, 1, length // dests, LANES), lambda s: (0, jnp.maximum(s - 1, 0), 0, 0)
            ),
            head_block,
            head_block,
        ],
        out_shape=[
            jax.ShapeDtypeStruct((dests, seqs, length // dests, LANES), BF16), heads, heads
        ],
        scratch_shapes=[pltpu.VMEM((2, length + 2 * EDGE, LANES), F32)],
        compiler_params=params("arbitrary", mb=28),
        cost_estimate=pl.CostEstimate(
            flops=2 * rows * width * weight.shape[2],
            transcendentals=0,
            bytes_accessed=2 * rows * width,
        ),
        name="project",
    )(in_hbm(normed), before, after, gain.reshape(1, width), weight, taps, cosine, sine)


def band_bias(first, last):
    query = lax.broadcasted_iota(jnp.int32, (Q_BLOCK, SPAN), 0)
    key = lax.broadcasted_iota(jnp.int32, (Q_BLOCK, SPAN), 1)
    allowed = (key >= query) & (key <= query + 2 * WINDOW) & (key >= first) & (key < last)
    return jnp.where(allowed, 0.0, MASK_VALUE).astype(F32)


def attend_blocks(sink_ref, jobs):
    low = lax.broadcasted_iota(jnp.int32, (Q_BLOCK, LANES), 1) < HEAD_DIM
    low_both = lax.broadcasted_iota(jnp.int32, (2 * Q_BLOCK, LANES), 1) < HEAD_DIM
    diagonal = lax.broadcasted_iota(jnp.int32, (LANES, LANES), 0) == lax.broadcasted_iota(
        jnp.int32, (LANES, LANES), 1
    )
    is_first = lax.broadcasted_iota(jnp.int32, (2 * Q_BLOCK, 1), 0) < Q_BLOCK
    sink = jnp.where(is_first, sink_ref[0], sink_ref[1])

    def score(job):
        query, bias = job[0](), job[3]()
        swapped = pltpu.roll(query.astype(F32), HEAD_DIM, 1).astype(BF16)
        own = jnp.concatenate([query, swapped], 0)
        own = jnp.where(low_both, own, jnp.zeros_like(own))
        scores = lax.dot_general(
            own, job[1](), (((1,), (1,)), ((), ())), preferred_element_type=F32
        )
        return scores + jnp.concatenate([bias, bias], 0)

    def weigh(scores):
        top = jnp.maximum(jnp.max(scores, axis=-1, keepdims=True), sink)
        return top, jnp.exp(scores - top).astype(BF16)

    def blend(job, top, weights):
        both = jnp.dot(weights, job[2](), preferred_element_type=F32)
        swapped = pltpu.roll(both, HEAD_DIM, 1)
        total = jnp.where(low_both, both, swapped) + jnp.exp(sink - top)
        log_total = top + jnp.log(total)
        logs = [
            jnp.sum(
                jnp.where(diagonal, log_total[head * Q_BLOCK : (head + 1) * Q_BLOCK], 0.0),
                axis=0,
                keepdims=True,
            )
            for head in range(2)
        ]
        first = swapped[:Q_BLOCK] / total[:Q_BLOCK]
        second = both[Q_BLOCK:] / total[Q_BLOCK:]
        job[4](jnp.where(low, first, second).astype(BF16), logs)

    ahead, behind = score(jobs[0]), None
    for at, job in enumerate(jobs):
        scores = ahead
        if at + 1 < len(jobs):
            ahead = score(jobs[at + 1])
        top, weights = weigh(scores)
        if behind is not None:
            blend(jobs[at - 1], *behind)
        behind = top, weights
    blend(jobs[-1], *behind)


def with_ones(keys):
    in_low = lax.broadcasted_iota(jnp.int32, keys.shape, keys.ndim - 1) < HEAD_DIM
    return jnp.where(in_low, jnp.ones_like(keys), keys)


def inner_kernel(sink_ref, q_ref, kv_ref, out_ref, log_ref, one_ref, bias_ref):
    length = kv_ref.shape[1]

    @pl.when(pl.program_id(0) == 0)
    def _():
        bias_ref[...] = band_bias(0, SPAN)

    one_ref[...] = with_ones(kv_ref[0])

    def job(block):
        at = block * Q_BLOCK
        span = slice(at - WINDOW, at + Q_BLOCK + WINDOW)

        def store(out, logs):
            out_ref[block, 0] = out
            for head in range(2):
                log_ref[0, head : head + 1, at : at + Q_BLOCK] = logs[head]

        return (
            lambda: q_ref[0, at : at + Q_BLOCK, :],
            lambda: kv_ref[0, span, :],
            lambda: one_ref[span, :],
            lambda: bias_ref[...],
            store,
        )

    attend_blocks(sink_ref, [job(block) for block in range(1, length // Q_BLOCK - 1)])


def attend_inner(sink, query, kv, dests):
    seqs, length, _ = kv.shape
    whole = pl.BlockSpec((1, length, LANES), lambda s: (s, 0, 0))
    return pl.pallas_call(
        inner_kernel,
        grid=(seqs,),
        in_specs=[pl.BlockSpec(memory_space=pltpu.SMEM), whole, whole],
        out_specs=[
            pl.BlockSpec((dests, 1, length // dests, LANES), lambda s: (0, s, 0, 0)),
            pl.BlockSpec((1, 2, length), lambda s: (s, 0, 0)),
        ],
        out_shape=[
            pltpu.HBM((dests, seqs, length // dests, LANES), BF16),
            pltpu.HBM((seqs, 2, length), F32),
        ],
        scratch_shapes=[
            pltpu.VMEM((length, LANES), BF16),
            pltpu.VMEM((Q_BLOCK, SPAN), F32),
        ],
        compiler_params=params("arbitrary", mb=28),
        cost_estimate=pl.CostEstimate(
            flops=40 * seqs * length * SPAN * LANES // 8,
            transcendentals=0,
            bytes_accessed=6 * seqs * length * LANES,
        ),
        name="attend_inner",
    )(sink, in_hbm(query), in_hbm(kv))


def edge_kernel(
    place_ref, sink_ref, q_low_ref, q_high_ref, before_ref, kv_low_ref, kv_high_ref, after_ref,
    _, __, out_ref, log_ref, pad_ref, one_ref, bias_ref, own_ref, own_log_ref, sems
):
    seqs = before_ref.shape[0]
    blocks = out_ref.shape[0]
    bias_ref[0] = band_bias(jnp.where(place_ref[0] == 0, WINDOW, 0), SPAN)
    bias_ref[1] = band_bias(
        0, jnp.where(place_ref[0] == place_ref[1] - 1, Q_BLOCK + WINDOW, SPAN)
    )
    pad_ref[0, :, :WINDOW] = before_ref[...]
    pad_ref[0, :, WINDOW:] = kv_low_ref[...]
    pad_ref[1, :, : SPAN - WINDOW] = kv_high_ref[...]
    pad_ref[1, :, SPAN - WINDOW :] = after_ref[...]
    one_ref[...] = with_ones(pad_ref[...])

    def job(side, seq):
        def store(out, logs):
            own_ref[side, seq] = out
            for head in range(2):
                own_log_ref[side, seq, head : head + 1, :] = logs[head]

        return (
            lambda: (q_low_ref, q_high_ref)[side][seq],
            lambda: pad_ref[side, seq],
            lambda: one_ref[side, seq],
            lambda: bias_ref[side],
            store,
        )

    attend_blocks(sink_ref, [job(side, seq) for side in range(2) for seq in range(seqs)])
    copies = []
    for side, block in enumerate((0, blocks - 1)):
        copies.append(
            pltpu.make_async_copy(own_ref.at[side], out_ref.at[block], sems.at[side, 0])
        )
        copies.append(
            pltpu.make_async_copy(
                own_log_ref.at[side],
                log_ref.at[:, :, pl.ds(block * Q_BLOCK, Q_BLOCK)],
                sems.at[side, 1],
            )
        )
    for copy in copies:
        copy.start()
    for copy in copies:
        copy.wait()


def attend_edge(place, sink, query, before, kv, after, out, log_total):
    seqs, length, _ = kv.shape
    ends = SPAN - WINDOW
    smem = pl.BlockSpec(memory_space=pltpu.SMEM)
    raw = pl.BlockSpec(memory_space=pl.ANY)

    def rows(count, at):
        return pl.BlockSpec((seqs, count, LANES), lambda i: (0, at, 0))

    return pl.pallas_call(
        edge_kernel,
        grid=(1,),
        in_specs=[
            smem,
            smem,
            rows(Q_BLOCK, 0),
            rows(Q_BLOCK, length // Q_BLOCK - 1),
            rows(WINDOW, 0),
            rows(ends, 0),
            rows(ends, length // ends - 1),
            rows(WINDOW, 0),
            raw,
            raw,
        ],
        out_specs=[raw, raw],
        out_shape=[pltpu.HBM(out.shape, BF16), pltpu.HBM(log_total.shape, F32)],
        input_output_aliases={8: 0, 9: 1},
        scratch_shapes=[
            pltpu.VMEM((2, seqs, SPAN, LANES), BF16),
            pltpu.VMEM((2, seqs, SPAN, LANES), BF16),
            pltpu.VMEM((2, Q_BLOCK, SPAN), F32),
            pltpu.VMEM((2, seqs, Q_BLOCK, LANES), BF16),
            pltpu.VMEM((2, seqs, 2, Q_BLOCK), F32),
            pltpu.SemaphoreType.DMA((2, 2)),
        ],
        compiler_params=params("arbitrary", mb=28),
        cost_estimate=pl.CostEstimate(
            flops=10 * seqs * length * SPAN * LANES // 8,
            transcendentals=0,
            bytes_accessed=2 * seqs * length * LANES,
        ),
        name="attend_edge",
    )(place, sink, in_hbm(query), in_hbm(query), before, in_hbm(kv), in_hbm(kv), after,
      in_hbm(out), in_hbm(log_total))


def side_by_side(ref):
    return jnp.concatenate([ref[i] for i in range(ref.shape[0])], axis=-1)


def columns(ref):
    return jnp.concatenate([ref[c].reshape(-1, LANES) for c in range(ref.shape[0])], axis=-1)


def mix_conv_kernel(x_ref, gain_ref, w_ref, out_ref, act_ref):
    @pl.when(pl.program_id(0) == 0)
    def _():
        v = normalize(side_by_side(x_ref), side_by_side(gain_ref)[0:1])
        act_ref[...] = (v / (1.0 + jnp.exp(-v))).astype(BF16)

    out_ref[...] = jnp.dot(act_ref[...], columns(w_ref), preferred_element_type=F32)


def mix_attn_kernel(x_ref, part_ref, w_ref, out_ref):
    total = part_ref[...] + jnp.dot(
        side_by_side(x_ref), columns(w_ref), preferred_element_type=F32
    )
    out_ref[...] = total.astype(BF16)


def mix(kernel, x, extra, weight, which, out_dtype, cols, name, scratch=()):
    sources, rows, _ = x.shape
    groups = weight.shape[0]
    block = pl.BlockSpec((rows, cols * LANES), lambda n: (0, n))
    if which == 0:
        place = weight.shape[2] // EDGE - 1
        extra_spec = pl.BlockSpec((None, sources, EDGE, LANES), lambda n: (0, 0, place, 0))
    else:
        extra_spec = block
    return pl.pallas_call(
        kernel,
        grid=(groups // cols,),
        in_specs=[
            pl.BlockSpec(x.shape, lambda n: (0, 0, 0)),
            extra_spec,
            pl.BlockSpec((cols, sources, LANES, LANES), lambda n: (n, 0, which, 0)),
        ],
        out_specs=block,
        out_shape=pltpu.HBM((rows, groups * LANES), out_dtype),
        scratch_shapes=list(scratch),
        compiler_params=params("arbitrary", mb=32),
        cost_estimate=pl.CostEstimate(
            flops=2 * rows * sources * LANES * groups * LANES,
            transcendentals=0,
            bytes_accessed=weight.size,
        ),
        name=name,
    )(x, extra, weight)


def pack_kernel(
    value_ref, gate_ref, query_ref, key_ref, kv_ref, conv_ref, attn_ref, gain_ref, out_ref, in_ref
):
    out_ref[0:LANES, :] = conv_ref[...]
    out_ref[LANES : 2 * LANES, :] = attn_ref[...]
    out_ref[2 * LANES :, :] = jnp.broadcast_to(gain_ref[...].astype(F32), (EDGE, LANES)).astype(BF16)
    both = jnp.concatenate([key_ref[...], kv_ref[...]], 0).astype(F32).T.astype(BF16)
    piece = jnp.concatenate([value_ref[...], gate_ref[...], query_ref[...], both], axis=1)
    for copy in range(in_ref.shape[0]):
        in_ref[copy] = piece


def pack(value, gate, query, key, kv, conv, attn, gain, copies):
    rows = value.shape[0]
    cols = 3 * LANES + 2 * key.shape[1]
    operands = (value, gate, query, key.T, kv.T, conv, attn, gain.reshape(1, LANES))
    shapes = ((2 * LANES + EDGE, LANES), (copies, rows, cols))
    return pl.pallas_call(
        pack_kernel,
        grid=(1,),
        in_specs=[pl.BlockSpec(a.shape, lambda i: (0, 0)) for a in operands],
        out_specs=[
            pl.BlockSpec(shapes[0], lambda i: (0, 0)),
            pl.BlockSpec(shapes[1], lambda i: (0, 0, 0)),
        ],
        out_shape=[
            jax.ShapeDtypeStruct(shapes[0], BF16),
            jax.ShapeDtypeStruct(shapes[1], BF16),
        ],
        compiler_params=pltpu.CompilerParams(vmem_limit_bytes=16 * 1024 * 1024),
        name="pack",
    )(*(in_hbm(a) for a in operands))


def turn_tables(tok_count):
    half = HEAD_DIM // 2
    offset = lax.axis_index("sp") * tok_count
    positions = (offset + jnp.arange(tok_count, dtype=jnp.int32)).astype(F32)
    lane = jnp.arange(LANES, dtype=jnp.int32)
    inverse = ROPE_BASE ** (-(lane % half).astype(F32) / half)
    angles = positions[:, None] * inverse[None, :]
    sign = jnp.where(lane % HEAD_DIM < half, -1.0, 1.0).astype(F32)[None, :]
    return jnp.cos(angles), jnp.sin(angles) * sign


def on_device(
    tokens,
    norm_gain,
    conv_value_weight,
    conv_gate_weight,
    query_weight,
    key_weight,
    value_weight,
    conv_taps,
    conv_gain,
    sink_logit,
    out_conv_weight,
    out_attn_weight,
):
    seqs, length, width = tokens.shape
    sp, tp = lax.axis_size("sp"), lax.axis_size("tp")
    place = jnp.stack([lax.axis_index("sp"), jnp.int32(sp)]).astype(jnp.int32)
    up = [(i, i + 1) for i in range(sp - 1)]
    down = [(i + 1, i) for i in range(sp - 1)]

    out_piece, in_piece = pack(
        conv_value_weight, conv_gate_weight, query_weight, key_weight, value_weight,
        out_conv_weight, out_attn_weight, conv_gain, sp,
    )
    out_weight = lax.all_gather(out_piece, ("sp", "tp"), axis=0, tiled=True)
    out_weight = out_weight.reshape(sp, tp, out_piece.shape[0], LANES)
    in_weight = lax.all_to_all(in_piece, "sp", 0, 0, tiled=True)

    before = lax.ppermute(tokens[:, -EDGE:], "sp", up)
    after = lax.ppermute(tokens[:, :EDGE], "sp", down)
    normed = norm_tokens(tokens.reshape(seqs * length, width), norm_gain)
    cosine, sine = turn_tables(length)
    filtered, query, kv = project(
        normed, before, after, norm_gain, in_weight, conv_taps, cosine, sine, tp
    )

    before = lax.ppermute(kv[:, -WINDOW:], "sp", up)
    after = lax.ppermute(kv[:, :WINDOW], "sp", down)
    conv_tok = lax.all_to_all(filtered, "tp", 0, 0, tiled=True)
    attn, log_total = attend_inner(sink_logit, query, kv, tp)
    attn, log_total = attend_edge(
        place, sink_logit, query, before, kv, after, attn, log_total
    )
    attn_tok = lax.all_to_all(attn, "tp", 0, 0, tiled=True)

    rows = seqs * length // tp
    out_weight = in_hbm(out_weight)
    part = mix(
        mix_conv_kernel, conv_tok.reshape(tp, rows, LANES), out_weight, out_weight, 0, F32, 4,
        "mix_conv", [pltpu.VMEM((rows, tp * LANES), BF16)],
    )
    mixed = mix(
        mix_attn_kernel, attn_tok.reshape(tp, rows, LANES), in_hbm(part), out_weight, 1, BF16, 8, "mix_attn"
    )
    return mixed.reshape(seqs, length // tp, width), log_total


def solution(mesh):
    placed = (
        P(None, "sp", None),
        P(),
        P("sp", "tp"),
        P("sp", "tp"),
        P("sp", "tp"),
        P("sp", "tp"),
        P("sp", "tp"),
        P(None, "tp"),
        P("tp"),
        P("tp"),
        P("tp", "sp"),
        P("tp", "sp"),
    )
    return jax.shard_map(
        on_device,
        mesh=mesh,
        in_specs=placed,
        out_specs=(P(None, ("sp", "tp"), None), P(None, "tp", "sp")),
        check_vma=False,
    )
```

```python
import functools

import jax
import jax.numpy as jnp
from jax import lax
from jax.experimental import pallas as pl
from jax.experimental.pallas import tpu as pltpu
from jax.sharding import PartitionSpec as P

HEAD_DIM = 64
WINDOW = 128
EPSILON = 1e-06
ROPE_BASE = 10000.0
MASK_VALUE = -1e30
LANES = 128
EDGE = 16
Q_BLOCK = 128
SPAN = Q_BLOCK + 2 * WINDOW
BF16 = jnp.bfloat16
F32 = jnp.float32


def in_hbm(value):
    return pltpu.with_memory_space_constraint(value, pltpu.HBM)


def params(*semantics, mb=48):
    return pltpu.CompilerParams(
        dimension_semantics=semantics, vmem_limit_bytes=mb * 1024 * 1024
    )


def normalize(x, gain):
    x = x.astype(F32)
    mean = jnp.mean(x, axis=-1, keepdims=True)
    centred = x - mean
    variance = jnp.mean(centred * centred, axis=-1, keepdims=True)
    return centred * lax.rsqrt(variance + EPSILON) * gain.astype(F32)


def norm_kernel(x_ref, gain_ref, out_ref):
    out_ref[...] = normalize(x_ref[...], gain_ref[...]).astype(BF16)


def norm_tokens(x, gain, block=512):
    rows, width = x.shape
    block = min(block, rows)
    return pl.pallas_call(
        norm_kernel,
        grid=(rows // block,),
        in_specs=[
            pl.BlockSpec((block, width), lambda i: (i, 0)),
            pl.BlockSpec((1, width), lambda i: (0, 0)),
        ],
        out_specs=pl.BlockSpec((block, width), lambda i: (i, 0)),
        out_shape=pltpu.HBM((rows, width), BF16),
        compiler_params=params("arbitrary", mb=28),
        cost_estimate=pl.CostEstimate(
            flops=40 * rows * width, transcendentals=rows, bytes_accessed=4 * rows * width
        ),
        name="norm_tokens",
    )(in_hbm(x), gain.reshape(1, width))


def project_kernel(
    x_ref, before_ref, after_ref, gain_ref, w_ref, taps_ref, cos_ref, sin_ref, out_ref, q_ref, kv_ref,
    low_ref, high_ref, buf_ref, *, sub, chunk
):
    step = pl.program_id(0)
    dests, _, share, _ = out_ref.shape
    length, seqs = dests * share, before_ref.shape[0]
    half = HEAD_DIM // 2
    tap_count = taps_ref.shape[0]
    shift = EDGE - tap_count // 2
    slot, last = step % 2, (step + 1) % 2
    taps = taps_ref[...].astype(F32)

    def gate(raw):
        return raw[:, :LANES] * jax.nn.sigmoid(raw[:, LANES : 2 * LANES])

    def filter_rows(first):
        for at in range(first, first + sub, chunk):
            total = jnp.zeros((chunk, LANES), F32)
            for tap in range(tap_count):
                rows = buf_ref[last, at + shift + tap : at + shift + tap + chunk, :]
                total = total + rows * taps[tap : tap + 1, :]
            out_ref[at // share, 0, at % share : at % share + chunk, :] = total.astype(BF16)

    @pl.when(step < seqs)
    def _():
        weight = w_ref[...].reshape(-1, w_ref.shape[2])
        lane = lax.broadcasted_iota(jnp.int32, (sub, LANES), 1)
        low, keyed = (lane % HEAD_DIM) < half, lane < HEAD_DIM
        edges = jnp.concatenate([before_ref[step], after_ref[step]], axis=0)
        edges = normalize(edges, gain_ref[...]).astype(BF16)
        ends = gate(
            jnp.dot(edges, weight[:, : 2 * LANES], preferred_element_type=F32)
        ).astype(BF16).astype(F32)
        buf_ref[slot, 0:EDGE, :] = ends[:EDGE]
        buf_ref[slot, EDGE + length : 2 * EDGE + length, :] = ends[EDGE:]
        for first in range(0, length, sub):
            raw = jnp.dot(x_ref[first : first + sub, :], weight, preferred_element_type=F32)
            filter_rows(first)
            buf_ref[slot, EDGE + first : EDGE + first + sub, :] = (
                gate(raw).astype(BF16).astype(F32)
            )
            table = slice(first, first + sub)
            for part, ref, scale in ((2, q_ref, HEAD_DIM**-0.5), (3, kv_ref, None)):
                x = raw[:, part * LANES : (part + 1) * LANES]
                partner = jnp.where(low, pltpu.roll(x, LANES - half, 1), pltpu.roll(x, half, 1))
                cosine, sine = cos_ref[table, :], sin_ref[table, :]
                if part == 3:
                    cosine, sine = jnp.where(keyed, cosine, 1.0), jnp.where(keyed, sine, 0.0)
                turned = x * cosine + partner * sine
                if scale is not None:
                    turned = turned * scale
                turned = turned.astype(BF16)
                ref[0, table, :] = turned
                if part == 3 and first == 0:
                    low_ref[step] = turned[:WINDOW]
                if part == 3 and first + sub == length:
                    high_ref[step] = turned[sub - WINDOW :]

    @pl.when(step == seqs)
    def _():
        for first in range(0, length, sub):
            filter_rows(first)


def project(normed, before, after, gain, weight, taps, cosine, sine, dests, sub=256, chunk=32):
    seqs = before.shape[0]
    rows, width = normed.shape
    length = rows // seqs
    inside = pl.BlockSpec(memory_space=pltpu.VMEM)
    heads = pltpu.HBM((seqs, length, LANES), BF16)
    head_block = pl.BlockSpec((1, length, LANES), lambda s: (jnp.minimum(s, seqs - 1), 0, 0))
    return pl.pallas_call(
        functools.partial(project_kernel, sub=sub, chunk=chunk),
        grid=(seqs + 1,),
        in_specs=[pl.BlockSpec((length, width), lambda s: (jnp.minimum(s, seqs - 1), 0))]
        + [inside] * 7,
        out_specs=[
            pl.BlockSpec(
                (dests, 1, length // dests, LANES), lambda s: (0, jnp.maximum(s - 1, 0), 0, 0)
            ),
            head_block,
            head_block,
            inside,
            inside,
        ],
        out_shape=[
            jax.ShapeDtypeStruct((dests, seqs, length // dests, LANES), BF16), heads, heads
        ]
        + [jax.ShapeDtypeStruct((seqs, WINDOW, LANES), BF16)] * 2,
        scratch_shapes=[pltpu.VMEM((2, length + 2 * EDGE, LANES), F32)],
        compiler_params=params("arbitrary", mb=28),
        cost_estimate=pl.CostEstimate(
            flops=2 * rows * width * weight.shape[2],
            transcendentals=0,
            bytes_accessed=2 * rows * width,
        ),
        name="project",
    )(in_hbm(normed), before, after, gain.reshape(1, width), weight, taps, cosine, sine)


def band_bias(first, last):
    query = lax.broadcasted_iota(jnp.int32, (Q_BLOCK, SPAN), 0)
    key = lax.broadcasted_iota(jnp.int32, (Q_BLOCK, SPAN), 1)
    allowed = (key >= query) & (key <= query + 2 * WINDOW) & (key >= first) & (key < last)
    return jnp.where(allowed, 0.0, MASK_VALUE).astype(F32)


def attend_blocks(sink_ref, jobs):
    low = lax.broadcasted_iota(jnp.int32, (Q_BLOCK, LANES), 1) < HEAD_DIM
    low_both = lax.broadcasted_iota(jnp.int32, (2 * Q_BLOCK, LANES), 1) < HEAD_DIM
    diagonal = lax.broadcasted_iota(jnp.int32, (LANES, LANES), 0) == lax.broadcasted_iota(
        jnp.int32, (LANES, LANES), 1
    )
    is_first = lax.broadcasted_iota(jnp.int32, (2 * Q_BLOCK, 1), 0) < Q_BLOCK
    sink = jnp.where(is_first, sink_ref[0], sink_ref[1])

    def score(job):
        query, bias = job[0](), job[3]()
        swapped = pltpu.roll(query.astype(F32), HEAD_DIM, 1).astype(BF16)
        own = jnp.concatenate([query, swapped], 0)
        own = jnp.where(low_both, own, jnp.zeros_like(own))
        scores = lax.dot_general(
            own, job[1](), (((1,), (1,)), ((), ())), preferred_element_type=F32
        )
        return scores + jnp.concatenate([bias, bias], 0)

    def weigh(scores):
        top = jnp.maximum(jnp.max(scores, axis=-1, keepdims=True), sink)
        return top, jnp.exp(scores - top).astype(BF16)

    def blend(job, top, weights):
        both = jnp.dot(weights, job[2](), preferred_element_type=F32)
        swapped = pltpu.roll(both, HEAD_DIM, 1)
        total = jnp.where(low_both, both, swapped) + jnp.exp(sink - top)
        log_total = top + jnp.log(total)
        logs = [
            jnp.sum(
                jnp.where(diagonal, log_total[head * Q_BLOCK : (head + 1) * Q_BLOCK], 0.0),
                axis=0,
                keepdims=True,
            )
            for head in range(2)
        ]
        first = swapped[:Q_BLOCK] / total[:Q_BLOCK]
        second = both[Q_BLOCK:] / total[Q_BLOCK:]
        job[4](jnp.where(low, first, second).astype(BF16), logs)

    ahead, behind = score(jobs[0]), None
    for at, job in enumerate(jobs):
        scores = ahead
        if at + 1 < len(jobs):
            ahead = score(jobs[at + 1])
        top, weights = weigh(scores)
        if behind is not None:
            blend(jobs[at - 1], *behind)
        behind = top, weights
    blend(jobs[-1], *behind)


def with_ones(keys):
    in_low = lax.broadcasted_iota(jnp.int32, keys.shape, keys.ndim - 1) < HEAD_DIM
    return jnp.where(in_low, jnp.ones_like(keys), keys)


def inner_kernel(sink_ref, q_ref, kv_ref, out_ref, log_ref, one_ref, bias_ref):
    length = kv_ref.shape[1]

    @pl.when(pl.program_id(0) == 0)
    def _():
        bias_ref[...] = band_bias(0, SPAN)

    one_ref[...] = with_ones(kv_ref[0])

    def job(block):
        at = block * Q_BLOCK
        span = slice(at - WINDOW, at + Q_BLOCK + WINDOW)

        def store(out, logs):
            out_ref[block, 0] = out
            for head in range(2):
                log_ref[0, head : head + 1, at : at + Q_BLOCK] = logs[head]

        return (
            lambda: q_ref[0, at : at + Q_BLOCK, :],
            lambda: kv_ref[0, span, :],
            lambda: one_ref[span, :],
            lambda: bias_ref[...],
            store,
        )

    attend_blocks(sink_ref, [job(block) for block in range(1, length // Q_BLOCK - 1)])


def attend_inner(sink, query, kv, dests):
    seqs, length, _ = kv.shape
    whole = pl.BlockSpec((1, length, LANES), lambda s: (s, 0, 0))
    return pl.pallas_call(
        inner_kernel,
        grid=(seqs,),
        in_specs=[pl.BlockSpec(memory_space=pltpu.SMEM), whole, whole],
        out_specs=[
            pl.BlockSpec((dests, 1, length // dests, LANES), lambda s: (0, s, 0, 0)),
            pl.BlockSpec((1, 2, length), lambda s: (s, 0, 0)),
        ],
        out_shape=[
            pltpu.HBM((dests, seqs, length // dests, LANES), BF16),
            pltpu.HBM((seqs, 2, length), F32),
        ],
        scratch_shapes=[
            pltpu.VMEM((length, LANES), BF16),
            pltpu.VMEM((Q_BLOCK, SPAN), F32),
        ],
        compiler_params=params("arbitrary", mb=28),
        cost_estimate=pl.CostEstimate(
            flops=40 * seqs * length * SPAN * LANES // 8,
            transcendentals=0,
            bytes_accessed=6 * seqs * length * LANES,
        ),
        name="attend_inner",
    )(sink, in_hbm(query), in_hbm(kv))


def edge_kernel(
    place_ref, sink_ref, q_low_ref, q_high_ref, before_ref, kv_low_ref, kv_high_ref, after_ref,
    _, __, out_ref, log_ref, pad_ref, one_ref, bias_ref, own_ref, own_log_ref, sems
):
    seqs = before_ref.shape[0]
    blocks = out_ref.shape[0]
    bias_ref[0] = band_bias(jnp.where(place_ref[0] == 0, WINDOW, 0), SPAN)
    bias_ref[1] = band_bias(
        0, jnp.where(place_ref[0] == place_ref[1] - 1, Q_BLOCK + WINDOW, SPAN)
    )
    pad_ref[0, :, :WINDOW] = before_ref[...]
    pad_ref[0, :, WINDOW:] = kv_low_ref[...]
    pad_ref[1, :, : SPAN - WINDOW] = kv_high_ref[...]
    pad_ref[1, :, SPAN - WINDOW :] = after_ref[...]
    one_ref[...] = with_ones(pad_ref[...])

    def job(side, seq):
        def store(out, logs):
            own_ref[side, seq] = out
            for head in range(2):
                own_log_ref[side, seq, head : head + 1, :] = logs[head]

        return (
            lambda: (q_low_ref, q_high_ref)[side][seq],
            lambda: pad_ref[side, seq],
            lambda: one_ref[side, seq],
            lambda: bias_ref[side],
            store,
        )

    attend_blocks(sink_ref, [job(side, seq) for side in range(2) for seq in range(seqs)])
    copies = []
    for side, block in enumerate((0, blocks - 1)):
        copies.append(
            pltpu.make_async_copy(own_ref.at[side], out_ref.at[block], sems.at[side, 0])
        )
        copies.append(
            pltpu.make_async_copy(
                own_log_ref.at[side],
                log_ref.at[:, :, pl.ds(block * Q_BLOCK, Q_BLOCK)],
                sems.at[side, 1],
            )
        )
    for copy in copies:
        copy.start()
    for copy in copies:
        copy.wait()


def attend_edge(place, sink, query, before, kv, after, out, log_total):
    seqs, length, _ = kv.shape
    ends = SPAN - WINDOW
    smem = pl.BlockSpec(memory_space=pltpu.SMEM)
    raw = pl.BlockSpec(memory_space=pl.ANY)

    def rows(count, at):
        return pl.BlockSpec((seqs, count, LANES), lambda i: (0, at, 0))

    return pl.pallas_call(
        edge_kernel,
        grid=(1,),
        in_specs=[
            smem,
            smem,
            rows(Q_BLOCK, 0),
            rows(Q_BLOCK, length // Q_BLOCK - 1),
            rows(WINDOW, 0),
            rows(ends, 0),
            rows(ends, length // ends - 1),
            rows(WINDOW, 0),
            raw,
            raw,
        ],
        out_specs=[raw, raw],
        out_shape=[pltpu.HBM(out.shape, BF16), pltpu.HBM(log_total.shape, F32)],
        input_output_aliases={8: 0, 9: 1},
        scratch_shapes=[
            pltpu.VMEM((2, seqs, SPAN, LANES), BF16),
            pltpu.VMEM((2, seqs, SPAN, LANES), BF16),
            pltpu.VMEM((2, Q_BLOCK, SPAN), F32),
            pltpu.VMEM((2, seqs, Q_BLOCK, LANES), BF16),
            pltpu.VMEM((2, seqs, 2, Q_BLOCK), F32),
            pltpu.SemaphoreType.DMA((2, 2)),
        ],
        compiler_params=params("arbitrary", mb=28),
        cost_estimate=pl.CostEstimate(
            flops=10 * seqs * length * SPAN * LANES // 8,
            transcendentals=0,
            bytes_accessed=2 * seqs * length * LANES,
        ),
        name="attend_edge",
    )(place, sink, in_hbm(query), in_hbm(query), before, in_hbm(kv), in_hbm(kv), after,
      in_hbm(out), in_hbm(log_total))


def side_by_side(ref):
    return jnp.concatenate([ref[i] for i in range(ref.shape[0])], axis=-1)


def by_core(ref, core):
    count = ref.shape[0] // 2
    own = [ref[2 * i + core] for i in range(count)]
    other = [ref[2 * i + 1 - core] for i in range(count)]
    return jnp.concatenate(own, axis=-1), jnp.concatenate(other, axis=-1)


def columns(ref):
    return jnp.concatenate([ref[c].reshape(-1, LANES) for c in range(ref.shape[0])], axis=-1)


def mix_conv_kernel(core_ref, x_ref, own_gain_ref, other_gain_ref, own_ref, other_ref, out_ref, act_ref):
    half = act_ref.shape[1] // 2

    @pl.when(pl.program_id(0) == 0)
    def _():
        x = jnp.concatenate(by_core(x_ref, core_ref[0]), axis=-1)
        gain = jnp.concatenate([side_by_side(own_gain_ref), side_by_side(other_gain_ref)], axis=-1)
        v = normalize(x, gain[0:1])
        act_ref[...] = (v / (1.0 + jnp.exp(-v))).astype(BF16)

    total = jnp.dot(act_ref[:, :half], columns(own_ref), preferred_element_type=F32)
    total = total + jnp.dot(act_ref[:, half:], columns(other_ref), preferred_element_type=F32)
    out_ref[...] = total


def mix_attn_kernel(core_ref, x_ref, part_ref, own_ref, other_ref, out_ref):
    own, other = by_core(x_ref, core_ref[0])
    total = part_ref[...] + jnp.dot(own, columns(own_ref), preferred_element_type=F32)
    total = total + jnp.dot(other, columns(other_ref), preferred_element_type=F32)
    out_ref[...] = total.astype(BF16)


def mix(kernel, core, x, extras, weights, which, out_dtype, cols, name, scratch=()):
    sources, rows, _ = x.shape
    groups, half, height, _ = weights[0].shape
    block = pl.BlockSpec((rows, cols * LANES), lambda n: (0, n))
    if which == 0:
        place = height // EDGE - 1
        extra_spec = pl.BlockSpec((None, half, EDGE, LANES), lambda n: (0, 0, place, 0))
    else:
        extra_spec = block
    return pl.pallas_call(
        kernel,
        grid=(groups // cols,),
        in_specs=[
            pl.BlockSpec(memory_space=pltpu.SMEM),
            pl.BlockSpec(x.shape, lambda n: (0, 0, 0)),
        ]
        + [extra_spec] * len(extras)
        + [pl.BlockSpec((cols, half, LANES, LANES), lambda n: (n, 0, which, 0))] * 2,
        out_specs=block,
        out_shape=pltpu.HBM((rows, groups * LANES), out_dtype),
        scratch_shapes=list(scratch),
        compiler_params=params("arbitrary", mb=32),
        cost_estimate=pl.CostEstimate(
            flops=2 * rows * sources * LANES * groups * LANES,
            transcendentals=0,
            bytes_accessed=2 * weights[0].size,
        ),
        name=name,
    )(core, x, *extras, *weights)


def pack_kernel(
    value_ref, gate_ref, query_ref, key_ref, kv_ref, conv_ref, attn_ref, gain_ref, out_ref, in_ref
):
    out_ref[0:LANES, :] = conv_ref[...]
    out_ref[LANES : 2 * LANES, :] = attn_ref[...]
    out_ref[2 * LANES :, :] = jnp.broadcast_to(gain_ref[...].astype(F32), (EDGE, LANES)).astype(BF16)
    both = jnp.concatenate([key_ref[...], kv_ref[...]], 0).astype(F32).T.astype(BF16)
    piece = jnp.concatenate([value_ref[...], gate_ref[...], query_ref[...], both], axis=1)
    for copy in range(in_ref.shape[0]):
        in_ref[copy] = piece


def pack(value, gate, query, key, kv, conv, attn, gain, copies):
    rows = value.shape[0]
    cols = 3 * LANES + 2 * key.shape[1]
    operands = (value, gate, query, key.T, kv.T, conv, attn, gain.reshape(1, LANES))
    shapes = ((2 * LANES + EDGE, LANES), (copies, rows, cols))
    return pl.pallas_call(
        pack_kernel,
        grid=(1,),
        in_specs=[pl.BlockSpec(a.shape, lambda i: (0, 0)) for a in operands],
        out_specs=[
            pl.BlockSpec(shapes[0], lambda i: (0, 0)),
            pl.BlockSpec(shapes[1], lambda i: (0, 0, 0)),
        ],
        out_shape=[
            jax.ShapeDtypeStruct(shapes[0], BF16),
            jax.ShapeDtypeStruct(shapes[1], BF16),
        ],
        compiler_params=pltpu.CompilerParams(vmem_limit_bytes=16 * 1024 * 1024),
        name="pack",
    )(*(in_hbm(a) for a in operands))


def turn_tables(tok_count):
    half = HEAD_DIM // 2
    offset = lax.axis_index("sp") * tok_count
    positions = (offset + jnp.arange(tok_count, dtype=jnp.int32)).astype(F32)
    lane = jnp.arange(LANES, dtype=jnp.int32)
    inverse = ROPE_BASE ** (-(lane % half).astype(F32) / half)
    angles = positions[:, None] * inverse[None, :]
    sign = jnp.where(lane % HEAD_DIM < half, -1.0, 1.0).astype(F32)[None, :]
    return jnp.cos(angles), jnp.sin(angles) * sign


def on_device(
    tokens,
    norm_gain,
    conv_value_weight,
    conv_gate_weight,
    query_weight,
    key_weight,
    value_weight,
    conv_taps,
    conv_gain,
    sink_logit,
    out_conv_weight,
    out_attn_weight,
):
    seqs, length, width = tokens.shape
    sp, tp = lax.axis_size("sp"), lax.axis_size("tp")
    place = jnp.stack([lax.axis_index("sp"), jnp.int32(sp)]).astype(jnp.int32)
    up = [(i, i + 1) for i in range(sp - 1)]
    down = [(i + 1, i) for i in range(sp - 1)]

    out_piece, in_piece = pack(
        conv_value_weight, conv_gate_weight, query_weight, key_weight, value_weight,
        out_conv_weight, out_attn_weight, conv_gain, sp,
    )
    same_core = [
        [row * tp + col for row in range(sp) for col in range(core, tp, 2)] for core in range(2)
    ]
    own_weight = lax.all_gather(
        out_piece, ("sp", "tp"), axis=0, tiled=True, axis_index_groups=same_core
    )
    in_weight = lax.all_to_all(in_piece, "sp", 0, 0, tiled=True)

    before = lax.ppermute(tokens[:, -EDGE:], "sp", up)
    after = lax.ppermute(tokens[:, :EDGE], "sp", down)
    normed = norm_tokens(tokens.reshape(seqs * length, width), norm_gain)
    cosine, sine = turn_tables(length)
    filtered, query, kv, low, high = project(
        normed, before, after, norm_gain, in_weight, conv_taps, cosine, sine, tp
    )

    before = lax.ppermute(high, "sp", up)
    after = lax.ppermute(low, "sp", down)
    conv_tok = lax.all_to_all(filtered, "tp", 0, 0, tiled=True)
    attn, log_total = attend_inner(sink_logit, query, kv, tp)
    attn, log_total = attend_edge(
        place, sink_logit, query, before, kv, after, attn, log_total
    )
    attn_tok = lax.all_to_all(attn, "tp", 0, 0, tiled=True)

    rows = seqs * length // tp
    own_weight, _ = lax.optimization_barrier((own_weight, log_total))
    other_weight = lax.ppermute(own_weight, "tp", [(i, i ^ 1) for i in range(tp)])
    weights = [
        in_hbm(w.reshape(sp, tp // 2, out_piece.shape[0], LANES))
        for w in (own_weight, other_weight)
    ]
    core = (lax.axis_index("tp") % 2).astype(jnp.int32).reshape(1)
    part = mix(
        mix_conv_kernel, core, conv_tok.reshape(tp, rows, LANES), weights, weights, 0, F32, 4,
        "mix_conv", [pltpu.VMEM((rows, tp * LANES), BF16)],
    )
    mixed = mix(
        mix_attn_kernel, core, attn_tok.reshape(tp, rows, LANES), [in_hbm(part)], weights, 1, BF16,
        4, "mix_attn",
    )
    return mixed.reshape(seqs, length // tp, width), log_total


def solution(mesh):
    placed = (
        P(None, "sp", None),
        P(),
        P("sp", "tp"),
        P("sp", "tp"),
        P("sp", "tp"),
        P("sp", "tp"),
        P("sp", "tp"),
        P(None, "tp"),
        P("tp"),
        P("tp"),
        P("tp", "sp"),
        P("tp", "sp"),
    )
    return jax.shard_map(
        on_device,
        mesh=mesh,
        in_specs=placed,
        out_specs=(P(None, ("sp", "tp"), None), P(None, "tp", "sp")),
        check_vma=False,
    )
```

```python
import functools

import jax
import jax.numpy as jnp
from jax import lax
from jax.experimental import pallas as pl
from jax.experimental.pallas import tpu as pltpu
from jax.sharding import PartitionSpec as P

HEAD_DIM = 64
WINDOW = 128
EPSILON = 1e-06
ROPE_BASE = 10000.0
MASK_VALUE = -1e30
LANES = 128
EDGE = 16
Q_BLOCK = 128
SPAN = Q_BLOCK + 2 * WINDOW
BF16 = jnp.bfloat16
F32 = jnp.float32


def in_hbm(value):
    return pltpu.with_memory_space_constraint(value, pltpu.HBM)


def params(*semantics, mb=48):
    return pltpu.CompilerParams(
        dimension_semantics=semantics, vmem_limit_bytes=mb * 1024 * 1024
    )


def normalize(x, gain):
    x = x.astype(F32)
    mean = jnp.mean(x, axis=-1, keepdims=True)
    centred = x - mean
    variance = jnp.mean(centred * centred, axis=-1, keepdims=True)
    return centred * lax.rsqrt(variance + EPSILON) * gain.astype(F32)


def norm_kernel(x_ref, gain_ref, out_ref):
    out_ref[...] = normalize(x_ref[...], gain_ref[...]).astype(BF16)


def norm_tokens(x, gain, block=512):
    rows, width = x.shape
    block = min(block, rows)
    return pl.pallas_call(
        norm_kernel,
        grid=(rows // block,),
        in_specs=[
            pl.BlockSpec((block, width), lambda i: (i, 0)),
            pl.BlockSpec((1, width), lambda i: (0, 0)),
        ],
        out_specs=pl.BlockSpec((block, width), lambda i: (i, 0)),
        out_shape=pltpu.HBM((rows, width), BF16),
        compiler_params=params("arbitrary", mb=28),
        cost_estimate=pl.CostEstimate(
            flops=40 * rows * width, transcendentals=rows, bytes_accessed=4 * rows * width
        ),
        name="norm_tokens",
    )(in_hbm(x), gain.reshape(1, width))


def project_kernel(
    x_ref, before_ref, after_ref, gain_ref, w_ref, taps_ref, cos_ref, sin_ref, out_ref, q_ref, kv_ref,
    low_ref, high_ref, buf_ref, *, sub, chunk
):
    step = pl.program_id(0)
    dests, _, share, _ = out_ref.shape
    length, seqs = dests * share, before_ref.shape[0]
    half = HEAD_DIM // 2
    tap_count = taps_ref.shape[0]
    shift = EDGE - tap_count // 2
    slot, last = step % 2, (step + 1) % 2
    taps = taps_ref[...].astype(F32)

    def gate(raw):
        return raw[:, :LANES] * jax.nn.sigmoid(raw[:, LANES : 2 * LANES])

    def filter_rows(first):
        for at in range(first, first + sub, chunk):
            total = jnp.zeros((chunk, LANES), F32)
            for tap in range(tap_count):
                rows = buf_ref[last, at + shift + tap : at + shift + tap + chunk, :]
                total = total + rows * taps[tap : tap + 1, :]
            out_ref[at // share, 0, at % share : at % share + chunk, :] = total.astype(BF16)

    @pl.when(step < seqs)
    def _():
        weight = w_ref[...].reshape(-1, w_ref.shape[2])
        lane = lax.broadcasted_iota(jnp.int32, (sub, LANES), 1)
        low, keyed = (lane % HEAD_DIM) < half, lane < HEAD_DIM
        edges = jnp.concatenate([before_ref[step], after_ref[step]], axis=0)
        edges = normalize(edges, gain_ref[...]).astype(BF16)
        ends = gate(
            jnp.dot(edges, weight[:, : 2 * LANES], preferred_element_type=F32)
        ).astype(BF16).astype(F32)
        buf_ref[slot, 0:EDGE, :] = ends[:EDGE]
        buf_ref[slot, EDGE + length : 2 * EDGE + length, :] = ends[EDGE:]
        for first in range(0, length, sub):
            raw = jnp.dot(x_ref[first : first + sub, :], weight, preferred_element_type=F32)
            filter_rows(first)
            buf_ref[slot, EDGE + first : EDGE + first + sub, :] = (
                gate(raw).astype(BF16).astype(F32)
            )
            table = slice(first, first + sub)
            for part, ref, scale in ((2, q_ref, HEAD_DIM**-0.5), (3, kv_ref, None)):
                x = raw[:, part * LANES : (part + 1) * LANES]
                partner = jnp.where(low, pltpu.roll(x, LANES - half, 1), pltpu.roll(x, half, 1))
                cosine, sine = cos_ref[table, :], sin_ref[table, :]
                if part == 3:
                    cosine, sine = jnp.where(keyed, cosine, 1.0), jnp.where(keyed, sine, 0.0)
                turned = x * cosine + partner * sine
                if scale is not None:
                    turned = turned * scale
                turned = turned.astype(BF16)
                ref[0, table, :] = turned
                if part == 3 and first == 0:
                    low_ref[step] = turned[:WINDOW]
                if part == 3 and first + sub == length:
                    high_ref[step] = turned[sub - WINDOW :]

    @pl.when(step == seqs)
    def _():
        for first in range(0, length, sub):
            filter_rows(first)


def project(normed, before, after, gain, weight, taps, cosine, sine, dests, sub=256, chunk=32):
    seqs = before.shape[0]
    rows, width = normed.shape
    length = rows // seqs
    inside = pl.BlockSpec(memory_space=pltpu.VMEM)
    heads = pltpu.HBM((seqs, length, LANES), BF16)
    head_block = pl.BlockSpec((1, length, LANES), lambda s: (jnp.minimum(s, seqs - 1), 0, 0))
    return pl.pallas_call(
        functools.partial(project_kernel, sub=sub, chunk=chunk),
        grid=(seqs + 1,),
        in_specs=[pl.BlockSpec((length, width), lambda s: (jnp.minimum(s, seqs - 1), 0))]
        + [inside] * 7,
        out_specs=[
            pl.BlockSpec(
                (dests, 1, length // dests, LANES), lambda s: (0, jnp.maximum(s - 1, 0), 0, 0)
            ),
            head_block,
            head_block,
            inside,
            inside,
        ],
        out_shape=[
            jax.ShapeDtypeStruct((dests, seqs, length // dests, LANES), BF16), heads, heads
        ]
        + [jax.ShapeDtypeStruct((seqs, WINDOW, LANES), BF16)] * 2,
        scratch_shapes=[pltpu.VMEM((2, length + 2 * EDGE, LANES), F32)],
        compiler_params=params("arbitrary", mb=28),
        cost_estimate=pl.CostEstimate(
            flops=2 * rows * width * weight.shape[2],
            transcendentals=0,
            bytes_accessed=2 * rows * width,
        ),
        name="project",
    )(in_hbm(normed), before, after, gain.reshape(1, width), weight, taps, cosine, sine)


def band_bias(first, last):
    query = lax.broadcasted_iota(jnp.int32, (Q_BLOCK, SPAN), 0)
    key = lax.broadcasted_iota(jnp.int32, (Q_BLOCK, SPAN), 1)
    allowed = (key >= query) & (key <= query + 2 * WINDOW) & (key >= first) & (key < last)
    return jnp.where(allowed, 0.0, MASK_VALUE).astype(F32)


def attend_blocks(sink_ref, jobs):
    low = lax.broadcasted_iota(jnp.int32, (Q_BLOCK, LANES), 1) < HEAD_DIM
    low_both = lax.broadcasted_iota(jnp.int32, (2 * Q_BLOCK, LANES), 1) < HEAD_DIM
    diagonal = lax.broadcasted_iota(jnp.int32, (LANES, LANES), 0) == lax.broadcasted_iota(
        jnp.int32, (LANES, LANES), 1
    )
    is_first = lax.broadcasted_iota(jnp.int32, (2 * Q_BLOCK, 1), 0) < Q_BLOCK
    sink = jnp.where(is_first, sink_ref[0], sink_ref[1])

    def score(job):
        query, bias = job[0](), job[3]()
        swapped = pltpu.roll(query.astype(F32), HEAD_DIM, 1).astype(BF16)
        own = jnp.concatenate([query, swapped], 0)
        own = jnp.where(low_both, own, jnp.zeros_like(own))
        scores = lax.dot_general(
            own, job[1](), (((1,), (1,)), ((), ())), preferred_element_type=F32
        )
        return scores + jnp.concatenate([bias, bias], 0)

    def weigh(scores):
        top = jnp.maximum(jnp.max(scores, axis=-1, keepdims=True), sink)
        return top, jnp.exp(scores - top).astype(BF16)

    def blend(job, top, weights):
        both = jnp.dot(weights, job[2](), preferred_element_type=F32)
        swapped = pltpu.roll(both, HEAD_DIM, 1)
        total = jnp.where(low_both, both, swapped) + jnp.exp(sink - top)
        log_total = top + jnp.log(total)
        logs = [
            jnp.sum(
                jnp.where(diagonal, log_total[head * Q_BLOCK : (head + 1) * Q_BLOCK], 0.0),
                axis=0,
                keepdims=True,
            )
            for head in range(2)
        ]
        first = swapped[:Q_BLOCK] / total[:Q_BLOCK]
        second = both[Q_BLOCK:] / total[Q_BLOCK:]
        job[4](jnp.where(low, first, second).astype(BF16), logs)

    ahead, behind = score(jobs[0]), None
    for at, job in enumerate(jobs):
        scores = ahead
        if at + 1 < len(jobs):
            ahead = score(jobs[at + 1])
        top, weights = weigh(scores)
        if behind is not None:
            blend(jobs[at - 1], *behind)
        behind = top, weights
    blend(jobs[-1], *behind)


def with_ones(keys):
    in_low = lax.broadcasted_iota(jnp.int32, keys.shape, keys.ndim - 1) < HEAD_DIM
    return jnp.where(in_low, jnp.ones_like(keys), keys)


def inner_kernel(sink_ref, q_ref, kv_ref, out_ref, log_ref, one_ref, bias_ref):
    length = kv_ref.shape[1]

    @pl.when(pl.program_id(0) == 0)
    def _():
        bias_ref[...] = band_bias(0, SPAN)

    one_ref[...] = with_ones(kv_ref[0])

    def job(block):
        at = block * Q_BLOCK
        span = slice(at - WINDOW, at + Q_BLOCK + WINDOW)

        def store(out, logs):
            out_ref[block, 0] = out
            for head in range(2):
                log_ref[0, head : head + 1, at : at + Q_BLOCK] = logs[head]

        return (
            lambda: q_ref[0, at : at + Q_BLOCK, :],
            lambda: kv_ref[0, span, :],
            lambda: one_ref[span, :],
            lambda: bias_ref[...],
            store,
        )

    attend_blocks(sink_ref, [job(block) for block in range(1, length // Q_BLOCK - 1)])


def attend_inner(sink, query, kv, dests):
    seqs, length, _ = kv.shape
    whole = pl.BlockSpec((1, length, LANES), lambda s: (s, 0, 0))
    return pl.pallas_call(
        inner_kernel,
        grid=(seqs,),
        in_specs=[pl.BlockSpec(memory_space=pltpu.SMEM), whole, whole],
        out_specs=[
            pl.BlockSpec((dests, 1, length // dests, LANES), lambda s: (0, s, 0, 0)),
            pl.BlockSpec((1, 2, length), lambda s: (s, 0, 0)),
        ],
        out_shape=[
            pltpu.HBM((dests, seqs, length // dests, LANES), BF16),
            pltpu.HBM((seqs, 2, length), F32),
        ],
        scratch_shapes=[
            pltpu.VMEM((length, LANES), BF16),
            pltpu.VMEM((Q_BLOCK, SPAN), F32),
        ],
        compiler_params=params("arbitrary", mb=28),
        cost_estimate=pl.CostEstimate(
            flops=40 * seqs * length * SPAN * LANES // 8,
            transcendentals=0,
            bytes_accessed=6 * seqs * length * LANES,
        ),
        name="attend_inner",
    )(sink, in_hbm(query), in_hbm(kv))


def edge_kernel(
    place_ref, sink_ref, q_low_ref, q_high_ref, before_ref, kv_low_ref, kv_high_ref, after_ref,
    _, __, out_ref, log_ref, pad_ref, one_ref, bias_ref, own_ref, own_log_ref, sems
):
    seqs = before_ref.shape[0]
    blocks = out_ref.shape[0]
    bias_ref[0] = band_bias(jnp.where(place_ref[0] == 0, WINDOW, 0), SPAN)
    bias_ref[1] = band_bias(
        0, jnp.where(place_ref[0] == place_ref[1] - 1, Q_BLOCK + WINDOW, SPAN)
    )
    pad_ref[0, :, :WINDOW] = before_ref[...]
    pad_ref[0, :, WINDOW:] = kv_low_ref[...]
    pad_ref[1, :, : SPAN - WINDOW] = kv_high_ref[...]
    pad_ref[1, :, SPAN - WINDOW :] = after_ref[...]
    one_ref[...] = with_ones(pad_ref[...])

    def job(side, seq):
        def store(out, logs):
            own_ref[side, seq] = out
            for head in range(2):
                own_log_ref[side, seq, head : head + 1, :] = logs[head]

        return (
            lambda: (q_low_ref, q_high_ref)[side][seq],
            lambda: pad_ref[side, seq],
            lambda: one_ref[side, seq],
            lambda: bias_ref[side],
            store,
        )

    attend_blocks(sink_ref, [job(side, seq) for side in range(2) for seq in range(seqs)])
    copies = []
    for side, block in enumerate((0, blocks - 1)):
        copies.append(
            pltpu.make_async_copy(own_ref.at[side], out_ref.at[block], sems.at[side, 0])
        )
        copies.append(
            pltpu.make_async_copy(
                own_log_ref.at[side],
                log_ref.at[:, :, pl.ds(block * Q_BLOCK, Q_BLOCK)],
                sems.at[side, 1],
            )
        )
    for copy in copies:
        copy.start()
    for copy in copies:
        copy.wait()


def attend_edge(place, sink, query, before, kv, after, out, log_total):
    seqs, length, _ = kv.shape
    ends = SPAN - WINDOW
    smem = pl.BlockSpec(memory_space=pltpu.SMEM)
    raw = pl.BlockSpec(memory_space=pl.ANY)

    def rows(count, at):
        return pl.BlockSpec((seqs, count, LANES), lambda i: (0, at, 0))

    return pl.pallas_call(
        edge_kernel,
        grid=(1,),
        in_specs=[
            smem,
            smem,
            rows(Q_BLOCK, 0),
            rows(Q_BLOCK, length // Q_BLOCK - 1),
            rows(WINDOW, 0),
            rows(ends, 0),
            rows(ends, length // ends - 1),
            rows(WINDOW, 0),
            raw,
            raw,
        ],
        out_specs=[raw, raw],
        out_shape=[pltpu.HBM(out.shape, BF16), pltpu.HBM(log_total.shape, F32)],
        input_output_aliases={8: 0, 9: 1},
        scratch_shapes=[
            pltpu.VMEM((2, seqs, SPAN, LANES), BF16),
            pltpu.VMEM((2, seqs, SPAN, LANES), BF16),
            pltpu.VMEM((2, Q_BLOCK, SPAN), F32),
            pltpu.VMEM((2, seqs, Q_BLOCK, LANES), BF16),
            pltpu.VMEM((2, seqs, 2, Q_BLOCK), F32),
            pltpu.SemaphoreType.DMA((2, 2)),
        ],
        compiler_params=params("arbitrary", mb=28),
        cost_estimate=pl.CostEstimate(
            flops=10 * seqs * length * SPAN * LANES // 8,
            transcendentals=0,
            bytes_accessed=2 * seqs * length * LANES,
        ),
        name="attend_edge",
    )(place, sink, in_hbm(query), in_hbm(query), before, in_hbm(kv), in_hbm(kv), after,
      in_hbm(out), in_hbm(log_total))


def side_by_side(ref):
    return jnp.concatenate([ref[i] for i in range(ref.shape[0])], axis=-1)


def by_core(ref, core):
    count = ref.shape[0] // 2
    own = [ref[2 * i + core] for i in range(count)]
    other = [ref[2 * i + 1 - core] for i in range(count)]
    return jnp.concatenate(own, axis=-1), jnp.concatenate(other, axis=-1)


def columns(ref):
    return jnp.concatenate([ref[c].reshape(-1, LANES) for c in range(ref.shape[0])], axis=-1)


def mix_conv_kernel(core_ref, x_ref, own_gain_ref, other_gain_ref, own_ref, other_ref, out_ref, act_ref):
    half = act_ref.shape[1] // 2

    @pl.when(pl.program_id(0) == 0)
    def _():
        x = jnp.concatenate(by_core(x_ref, core_ref[0]), axis=-1)
        gain = jnp.concatenate([side_by_side(own_gain_ref), side_by_side(other_gain_ref)], axis=-1)
        v = normalize(x, gain[0:1])
        act_ref[...] = (v / (1.0 + jnp.exp(-v))).astype(BF16)

    total = jnp.dot(act_ref[:, :half], columns(own_ref), preferred_element_type=F32)
    total = total + jnp.dot(act_ref[:, half:], columns(other_ref), preferred_element_type=F32)
    out_ref[...] = total


def mix_attn_kernel(core_ref, x_ref, part_ref, own_ref, other_ref, out_ref):
    own, other = by_core(x_ref, core_ref[0])
    total = part_ref[...] + jnp.dot(own, columns(own_ref), preferred_element_type=F32)
    total = total + jnp.dot(other, columns(other_ref), preferred_element_type=F32)
    out_ref[...] = total.astype(BF16)


def mix(kernel, core, x, extras, weights, which, out_dtype, cols, scratch=()):
    sources, rows, _ = x.shape
    groups, half, height, _ = weights[0].shape
    block = pl.BlockSpec((rows, cols * LANES), lambda n: (0, n))
    if which == 0:
        place = height // EDGE - 1
        extra_spec = pl.BlockSpec((None, half, EDGE, LANES), lambda n: (0, 0, place, 0))
    else:
        extra_spec = block
    return pl.pallas_call(
        kernel,
        grid=(groups // cols,),
        in_specs=[
            pl.BlockSpec(memory_space=pltpu.SMEM),
            pl.BlockSpec(x.shape, lambda n: (0, 0, 0)),
        ]
        + [extra_spec] * len(extras)
        + [pl.BlockSpec((cols, half, LANES, LANES), lambda n: (n, 0, which, 0))] * 2,
        out_specs=block,
        out_shape=pltpu.HBM((rows, groups * LANES), out_dtype),
        scratch_shapes=list(scratch),
        compiler_params=params("arbitrary", mb=32),
        cost_estimate=pl.CostEstimate(
            flops=2 * rows * sources * LANES * groups * LANES,
            transcendentals=0,
            bytes_accessed=2 * weights[0].size,
        ),
    )(core, x, *extras, *weights)


def pack_kernel(
    value_ref, gate_ref, query_ref, key_ref, kv_ref, conv_ref, attn_ref, gain_ref, out_ref, in_ref
):
    out_ref[0:LANES, :] = conv_ref[...]
    out_ref[LANES : 2 * LANES, :] = attn_ref[...]
    out_ref[2 * LANES :, :] = jnp.broadcast_to(gain_ref[...].astype(F32), (EDGE, LANES)).astype(BF16)
    both = jnp.concatenate([key_ref[...], kv_ref[...]], 0).astype(F32).T.astype(BF16)
    piece = jnp.concatenate([value_ref[...], gate_ref[...], query_ref[...], both], axis=1)
    for copy in range(in_ref.shape[0]):
        in_ref[copy] = piece


def pack(value, gate, query, key, kv, conv, attn, gain, copies):
    rows = value.shape[0]
    cols = 3 * LANES + 2 * key.shape[1]
    operands = (value, gate, query, key.T, kv.T, conv, attn, gain.reshape(1, LANES))
    shapes = ((2 * LANES + EDGE, LANES), (copies, rows, cols))
    return pl.pallas_call(
        pack_kernel,
        grid=(1,),
        in_specs=[pl.BlockSpec(a.shape, lambda i: (0, 0)) for a in operands],
        out_specs=[
            pl.BlockSpec(shapes[0], lambda i: (0, 0)),
            pl.BlockSpec(shapes[1], lambda i: (0, 0, 0)),
        ],
        out_shape=[
            jax.ShapeDtypeStruct(shapes[0], BF16),
            jax.ShapeDtypeStruct(shapes[1], BF16),
        ],
        compiler_params=pltpu.CompilerParams(vmem_limit_bytes=16 * 1024 * 1024),
        name="pack",
    )(*(in_hbm(a) for a in operands))


def turn_tables(tok_count):
    half = HEAD_DIM // 2
    offset = lax.axis_index("sp") * tok_count
    positions = (offset + jnp.arange(tok_count, dtype=jnp.int32)).astype(F32)
    lane = jnp.arange(LANES, dtype=jnp.int32)
    inverse = ROPE_BASE ** (-(lane % half).astype(F32) / half)
    angles = positions[:, None] * inverse[None, :]
    sign = jnp.where(lane % HEAD_DIM < half, -1.0, 1.0).astype(F32)[None, :]
    return jnp.cos(angles), jnp.sin(angles) * sign


def on_device(
    tokens,
    norm_gain,
    conv_value_weight,
    conv_gate_weight,
    query_weight,
    key_weight,
    value_weight,
    conv_taps,
    conv_gain,
    sink_logit,
    out_conv_weight,
    out_attn_weight,
):
    seqs, length, width = tokens.shape
    sp, tp = lax.axis_size("sp"), lax.axis_size("tp")
    place = jnp.stack([lax.axis_index("sp"), jnp.int32(sp)]).astype(jnp.int32)
    up = [(i, i + 1) for i in range(sp - 1)]
    down = [(i + 1, i) for i in range(sp - 1)]

    out_piece, in_piece = pack(
        conv_value_weight, conv_gate_weight, query_weight, key_weight, value_weight,
        out_conv_weight, out_attn_weight, conv_gain, sp,
    )
    same_core = [
        [row * tp + col for row in range(sp) for col in range(core, tp, 2)] for core in range(2)
    ]
    own_weight = lax.all_gather(
        out_piece, ("sp", "tp"), axis=0, tiled=True, axis_index_groups=same_core
    )
    in_weight = lax.all_to_all(in_piece, "sp", 0, 0, tiled=True)

    before = lax.ppermute(tokens[:, -EDGE:], "sp", up)
    after = lax.ppermute(tokens[:, :EDGE], "sp", down)
    normed = norm_tokens(tokens.reshape(seqs * length, width), norm_gain)
    cosine, sine = turn_tables(length)
    filtered, query, kv, low, high = project(
        normed, before, after, norm_gain, in_weight, conv_taps, cosine, sine, tp
    )

    before = lax.ppermute(high, "sp", up)
    after = lax.ppermute(low, "sp", down)
    conv_tok = lax.all_to_all(filtered, "tp", 0, 0, tiled=True)
    attn, log_total = attend_inner(sink_logit, query, kv, tp)
    attn, log_total = attend_edge(
        place, sink_logit, query, before, kv, after, attn, log_total
    )
    attn_tok = lax.all_to_all(attn, "tp", 0, 0, tiled=True)

    rows = seqs * length // tp
    own_weight, conv_tok, _ = lax.optimization_barrier((own_weight, conv_tok, log_total))
    other_weight = lax.ppermute(own_weight, "tp", [(i, i ^ 1) for i in range(tp)])
    weights = [
        in_hbm(w.reshape(sp, tp // 2, out_piece.shape[0], LANES))
        for w in (own_weight, other_weight)
    ]
    core = (lax.axis_index("tp") % 2).astype(jnp.int32).reshape(1)
    part = mix(
        mix_conv_kernel, core, conv_tok.reshape(tp, rows, LANES), weights, weights, 0, F32, 4,
        [pltpu.VMEM((rows, tp * LANES), BF16)],
    )
    mixed = mix(
        mix_attn_kernel, core, attn_tok.reshape(tp, rows, LANES), [in_hbm(part)], weights, 1, BF16,
        4,
    )
    return mixed.reshape(seqs, length // tp, width), log_total


def solution(mesh):
    placed = (
        P(None, "sp", None),
        P(),
        P("sp", "tp"),
        P("sp", "tp"),
        P("sp", "tp"),
        P("sp", "tp"),
        P("sp", "tp"),
        P(None, "tp"),
        P("tp"),
        P("tp"),
        P("tp", "sp"),
        P("tp", "sp"),
    )

    return jax.shard_map(
        on_device,
        mesh=mesh,
        in_specs=placed,
        out_specs=(P(None, ("sp", "tp"), None), P(None, "tp", "sp")),
        check_vma=False,
    )
```

```python
import functools

import jax
import jax.numpy as jnp
from jax import lax
from jax.experimental import pallas as pl
from jax.experimental.pallas import tpu as pltpu
from jax.sharding import PartitionSpec as P

HEAD_DIM = 64
WINDOW = 128
EPSILON = 1e-06
ROPE_BASE = 10000.0
MASK_VALUE = -1e30
LANES = 128
EDGE = 16
Q_BLOCK = 128
SPAN = Q_BLOCK + 2 * WINDOW
BF16 = jnp.bfloat16
F32 = jnp.float32


def in_hbm(value):
    return pltpu.with_memory_space_constraint(value, pltpu.HBM)


def params(*semantics, mb=48):
    return pltpu.CompilerParams(
        dimension_semantics=semantics, vmem_limit_bytes=mb * 1024 * 1024
    )


def normalize(x, gain):
    x = x.astype(F32)
    mean = jnp.mean(x, axis=-1, keepdims=True)
    centred = x - mean
    variance = jnp.mean(centred * centred, axis=-1, keepdims=True)
    return centred * lax.rsqrt(variance + EPSILON) * gain.astype(F32)


def norm_kernel(x_ref, gain_ref, out_ref):
    out_ref[...] = normalize(x_ref[...], gain_ref[...]).astype(BF16)


def norm_tokens(x, gain, block=512):
    rows, width = x.shape
    block = min(block, rows)
    return pl.pallas_call(
        norm_kernel,
        grid=(rows // block,),
        in_specs=[
            pl.BlockSpec((block, width), lambda i: (i, 0)),
            pl.BlockSpec((1, width), lambda i: (0, 0)),
        ],
        out_specs=pl.BlockSpec((block, width), lambda i: (i, 0)),
        out_shape=pltpu.HBM((rows, width), BF16),
        compiler_params=params("arbitrary", mb=28),
        cost_estimate=pl.CostEstimate(
            flops=40 * rows * width, transcendentals=rows, bytes_accessed=4 * rows * width
        ),
        name="norm_tokens",
    )(in_hbm(x), gain.reshape(1, width))


def project_kernel(
    x_ref, before_ref, after_ref, gain_ref, w_ref, taps_ref, cos_ref, sin_ref, out_ref, q_ref, kv_ref,
    low_ref, high_ref, buf_ref, *, sub, chunk
):
    step = pl.program_id(0)
    dests, _, share, _ = out_ref.shape
    length, seqs = dests * share, before_ref.shape[0]
    half = HEAD_DIM // 2
    tap_count = taps_ref.shape[0]
    shift = EDGE - tap_count // 2
    slot, last = step % 2, (step + 1) % 2
    taps = taps_ref[...].astype(F32)

    def gate(raw):
        return raw[:, :LANES] * jax.nn.sigmoid(raw[:, LANES : 2 * LANES])

    def filter_rows(first):
        for at in range(first, first + sub, chunk):
            total = jnp.zeros((chunk, LANES), F32)
            for tap in range(tap_count):
                rows = buf_ref[last, at + shift + tap : at + shift + tap + chunk, :]
                total = total + rows * taps[tap : tap + 1, :]
            out_ref[at // share, 0, at % share : at % share + chunk, :] = total.astype(BF16)

    @pl.when(step < seqs)
    def _():
        weight = w_ref[...].reshape(-1, w_ref.shape[2])
        lane = lax.broadcasted_iota(jnp.int32, (sub, LANES), 1)
        low, keyed = (lane % HEAD_DIM) < half, lane < HEAD_DIM
        edges = jnp.concatenate([before_ref[step], after_ref[step]], axis=0)
        edges = normalize(edges, gain_ref[...]).astype(BF16)
        ends = gate(
            jnp.dot(edges, weight[:, : 2 * LANES], preferred_element_type=F32)
        ).astype(BF16).astype(F32)
        buf_ref[slot, 0:EDGE, :] = ends[:EDGE]
        buf_ref[slot, EDGE + length : 2 * EDGE + length, :] = ends[EDGE:]
        for first in range(0, length, sub):
            raw = jnp.dot(x_ref[first : first + sub, :], weight, preferred_element_type=F32)
            filter_rows(first)
            buf_ref[slot, EDGE + first : EDGE + first + sub, :] = (
                gate(raw).astype(BF16).astype(F32)
            )
            table = slice(first, first + sub)
            for part, ref, scale in ((2, q_ref, HEAD_DIM**-0.5), (3, kv_ref, None)):
                x = raw[:, part * LANES : (part + 1) * LANES]
                partner = jnp.where(low, pltpu.roll(x, LANES - half, 1), pltpu.roll(x, half, 1))
                cosine, sine = cos_ref[table, :], sin_ref[table, :]
                if part == 3:
                    cosine, sine = jnp.where(keyed, cosine, 1.0), jnp.where(keyed, sine, 0.0)
                turned = x * cosine + partner * sine
                if scale is not None:
                    turned = turned * scale
                turned = turned.astype(BF16)
                ref[0, table, :] = turned
                if part == 3 and first == 0:
                    low_ref[step] = turned[:WINDOW]
                if part == 3 and first + sub == length:
                    high_ref[step] = turned[sub - WINDOW :]

    @pl.when(step == seqs)
    def _():
        for first in range(0, length, sub):
            filter_rows(first)


def project(normed, before, after, gain, weight, taps, cosine, sine, dests, sub=256, chunk=32):
    seqs = before.shape[0]
    rows, width = normed.shape
    length = rows // seqs
    inside = pl.BlockSpec(memory_space=pltpu.VMEM)
    heads = pltpu.HBM((seqs, length, LANES), BF16)
    head_block = pl.BlockSpec((1, length, LANES), lambda s: (jnp.minimum(s, seqs - 1), 0, 0))
    return pl.pallas_call(
        functools.partial(project_kernel, sub=sub, chunk=chunk),
        grid=(seqs + 1,),
        in_specs=[pl.BlockSpec((length, width), lambda s: (jnp.minimum(s, seqs - 1), 0))]
        + [inside] * 7,
        out_specs=[
            pl.BlockSpec(
                (dests, 1, length // dests, LANES), lambda s: (0, jnp.maximum(s - 1, 0), 0, 0)
            ),
            head_block,
            head_block,
            inside,
            inside,
        ],
        out_shape=[
            jax.ShapeDtypeStruct((dests, seqs, length // dests, LANES), BF16), heads, heads
        ]
        + [jax.ShapeDtypeStruct((seqs, WINDOW, LANES), BF16)] * 2,
        scratch_shapes=[pltpu.VMEM((2, length + 2 * EDGE, LANES), F32)],
        compiler_params=params("arbitrary", mb=28),
        cost_estimate=pl.CostEstimate(
            flops=2 * rows * width * weight.shape[2],
            transcendentals=0,
            bytes_accessed=2 * rows * width,
        ),
        name="project",
    )(in_hbm(normed), before, after, gain.reshape(1, width), weight, taps, cosine, sine)


def band_bias(first, last):
    query = lax.broadcasted_iota(jnp.int32, (Q_BLOCK, SPAN), 0)
    key = lax.broadcasted_iota(jnp.int32, (Q_BLOCK, SPAN), 1)
    allowed = (key >= query) & (key <= query + 2 * WINDOW) & (key >= first) & (key < last)
    return jnp.where(allowed, 0.0, MASK_VALUE).astype(F32)


def attend_blocks(sink_ref, jobs):
    low = lax.broadcasted_iota(jnp.int32, (Q_BLOCK, LANES), 1) < HEAD_DIM
    low_both = lax.broadcasted_iota(jnp.int32, (2 * Q_BLOCK, LANES), 1) < HEAD_DIM
    diagonal = lax.broadcasted_iota(jnp.int32, (LANES, LANES), 0) == lax.broadcasted_iota(
        jnp.int32, (LANES, LANES), 1
    )
    is_first = lax.broadcasted_iota(jnp.int32, (2 * Q_BLOCK, 1), 0) < Q_BLOCK
    sink = jnp.where(is_first, sink_ref[0], sink_ref[1])

    def score(job):
        query, bias = job[0](), job[3]()
        swapped = pltpu.roll(query.astype(F32), HEAD_DIM, 1).astype(BF16)
        own = jnp.concatenate([query, swapped], 0)
        own = jnp.where(low_both, own, jnp.zeros_like(own))
        scores = lax.dot_general(
            own, job[1](), (((1,), (1,)), ((), ())), preferred_element_type=F32
        )
        return scores + jnp.concatenate([bias, bias], 0)

    def weigh(scores):
        top = jnp.maximum(jnp.max(scores, axis=-1, keepdims=True), sink)
        return top, jnp.exp(scores - top).astype(BF16)

    def blend(job, top, weights):
        both = jnp.dot(weights, job[2](), preferred_element_type=F32)
        swapped = pltpu.roll(both, HEAD_DIM, 1)
        total = jnp.where(low_both, both, swapped) + jnp.exp(sink - top)
        log_total = top + jnp.log(total)
        logs = [
            jnp.sum(
                jnp.where(diagonal, log_total[head * Q_BLOCK : (head + 1) * Q_BLOCK], 0.0),
                axis=0,
                keepdims=True,
            )
            for head in range(2)
        ]
        first = swapped[:Q_BLOCK] / total[:Q_BLOCK]
        second = both[Q_BLOCK:] / total[Q_BLOCK:]
        job[4](jnp.where(low, first, second).astype(BF16), logs)

    ahead, behind = score(jobs[0]), None
    for at, job in enumerate(jobs):
        scores = ahead
        if at + 1 < len(jobs):
            ahead = score(jobs[at + 1])
        top, weights = weigh(scores)
        if behind is not None:
            blend(jobs[at - 1], *behind)
        behind = top, weights
    blend(jobs[-1], *behind)


def with_ones(keys):
    in_low = lax.broadcasted_iota(jnp.int32, keys.shape, keys.ndim - 1) < HEAD_DIM
    return jnp.where(in_low, jnp.ones_like(keys), keys)


def inner_kernel(sink_ref, q_ref, kv_ref, out_ref, log_ref, one_ref, bias_ref):
    length = kv_ref.shape[1]

    @pl.when(pl.program_id(0) == 0)
    def _():
        bias_ref[...] = band_bias(0, SPAN)

    one_ref[...] = with_ones(kv_ref[0])

    def job(block):
        at = block * Q_BLOCK
        span = slice(at - WINDOW, at + Q_BLOCK + WINDOW)

        def store(out, logs):
            out_ref[block, 0] = out
            for head in range(2):
                log_ref[0, head : head + 1, at : at + Q_BLOCK] = logs[head]

        return (
            lambda: q_ref[0, at : at + Q_BLOCK, :],
            lambda: kv_ref[0, span, :],
            lambda: one_ref[span, :],
            lambda: bias_ref[...],
            store,
        )

    attend_blocks(sink_ref, [job(block) for block in range(1, length // Q_BLOCK - 1)])


def attend_inner(sink, query, kv, dests):
    seqs, length, _ = kv.shape
    whole = pl.BlockSpec((1, length, LANES), lambda s: (s, 0, 0))
    return pl.pallas_call(
        inner_kernel,
        grid=(seqs,),
        in_specs=[pl.BlockSpec(memory_space=pltpu.SMEM), whole, whole],
        out_specs=[
            pl.BlockSpec((dests, 1, length // dests, LANES), lambda s: (0, s, 0, 0)),
            pl.BlockSpec((1, 2, length), lambda s: (s, 0, 0)),
        ],
        out_shape=[
            pltpu.HBM((dests, seqs, length // dests, LANES), BF16),
            pltpu.HBM((seqs, 2, length), F32),
        ],
        scratch_shapes=[
            pltpu.VMEM((length, LANES), BF16),
            pltpu.VMEM((Q_BLOCK, SPAN), F32),
        ],
        compiler_params=params("arbitrary", mb=28),
        cost_estimate=pl.CostEstimate(
            flops=40 * seqs * length * SPAN * LANES // 8,
            transcendentals=0,
            bytes_accessed=6 * seqs * length * LANES,
        ),
        name="attend_inner",
    )(sink, in_hbm(query), in_hbm(kv))


def edge_kernel(
    place_ref, sink_ref, q_low_ref, q_high_ref, before_ref, kv_low_ref, kv_high_ref, after_ref,
    _, __, out_ref, log_ref, pad_ref, one_ref, bias_ref, own_ref, own_log_ref, sems
):
    seqs = before_ref.shape[0]
    blocks = out_ref.shape[0]
    bias_ref[0] = band_bias(jnp.where(place_ref[0] == 0, WINDOW, 0), SPAN)
    bias_ref[1] = band_bias(
        0, jnp.where(place_ref[0] == place_ref[1] - 1, Q_BLOCK + WINDOW, SPAN)
    )
    pad_ref[0, :, :WINDOW] = before_ref[...]
    pad_ref[0, :, WINDOW:] = kv_low_ref[...]
    pad_ref[1, :, : SPAN - WINDOW] = kv_high_ref[...]
    pad_ref[1, :, SPAN - WINDOW :] = after_ref[...]
    one_ref[...] = with_ones(pad_ref[...])

    def job(side, seq):
        def store(out, logs):
            own_ref[side, seq] = out
            for head in range(2):
                own_log_ref[side, seq, head : head + 1, :] = logs[head]

        return (
            lambda: (q_low_ref, q_high_ref)[side][seq],
            lambda: pad_ref[side, seq],
            lambda: one_ref[side, seq],
            lambda: bias_ref[side],
            store,
        )

    attend_blocks(sink_ref, [job(side, seq) for side in range(2) for seq in range(seqs)])
    copies = []
    for side, block in enumerate((0, blocks - 1)):
        copies.append(
            pltpu.make_async_copy(own_ref.at[side], out_ref.at[block], sems.at[side, 0])
        )
        copies.append(
            pltpu.make_async_copy(
                own_log_ref.at[side],
                log_ref.at[:, :, pl.ds(block * Q_BLOCK, Q_BLOCK)],
                sems.at[side, 1],
            )
        )
    for copy in copies:
        copy.start()
    for copy in copies:
        copy.wait()


def attend_edge(place, sink, query, before, kv, after, out, log_total):
    seqs, length, _ = kv.shape
    ends = SPAN - WINDOW
    smem = pl.BlockSpec(memory_space=pltpu.SMEM)
    raw = pl.BlockSpec(memory_space=pl.ANY)

    def rows(count, at):
        return pl.BlockSpec((seqs, count, LANES), lambda i: (0, at, 0))

    return pl.pallas_call(
        edge_kernel,
        grid=(1,),
        in_specs=[
            smem,
            smem,
            rows(Q_BLOCK, 0),
            rows(Q_BLOCK, length // Q_BLOCK - 1),
            rows(WINDOW, 0),
            rows(ends, 0),
            rows(ends, length // ends - 1),
            rows(WINDOW, 0),
            raw,
            raw,
        ],
        out_specs=[raw, raw],
        out_shape=[pltpu.HBM(out.shape, BF16), pltpu.HBM(log_total.shape, F32)],
        input_output_aliases={8: 0, 9: 1},
        scratch_shapes=[
            pltpu.VMEM((2, seqs, SPAN, LANES), BF16),
            pltpu.VMEM((2, seqs, SPAN, LANES), BF16),
            pltpu.VMEM((2, Q_BLOCK, SPAN), F32),
            pltpu.VMEM((2, seqs, Q_BLOCK, LANES), BF16),
            pltpu.VMEM((2, seqs, 2, Q_BLOCK), F32),
            pltpu.SemaphoreType.DMA((2, 2)),
        ],
        compiler_params=params("arbitrary", mb=28),
        cost_estimate=pl.CostEstimate(
            flops=10 * seqs * length * SPAN * LANES // 8,
            transcendentals=0,
            bytes_accessed=2 * seqs * length * LANES,
        ),
        name="attend_edge",
    )(place, sink, in_hbm(query), in_hbm(query), before, in_hbm(kv), in_hbm(kv), after,
      in_hbm(out), in_hbm(log_total))


def side_by_side(ref):
    return jnp.concatenate([ref[i] for i in range(ref.shape[0])], axis=-1)


def by_core(ref, meta_ref):
    core, y = meta_ref[0], meta_ref[1]
    count = ref.shape[0] // 2
    places = [2 * ((y - step + count) % count) for step in range(count)]
    own = [ref[place + core] for place in places]
    other = [ref[place + 1 - core] for place in places]
    return jnp.concatenate(own, axis=-1), jnp.concatenate(other, axis=-1)


def columns(ref):
    return jnp.concatenate([ref[c].reshape(-1, LANES) for c in range(ref.shape[0])], axis=-1)


def product(rows, own_ref, other_ref):
    both = jnp.concatenate([columns(own_ref), columns(other_ref)], axis=0)
    return jnp.dot(rows, both, preferred_element_type=F32)


def mix_conv_kernel(
    meta_ref, x_ref, own_gain_ref, other_gain_ref, own_ref, other_ref, out_ref, act_ref
):
    @pl.when(pl.program_id(0) == 0)
    def _():
        x = jnp.concatenate(by_core(x_ref, meta_ref), axis=-1)
        gain = jnp.concatenate([side_by_side(own_gain_ref), side_by_side(other_gain_ref)], axis=-1)
        v = normalize(x, gain[0:1])
        act_ref[...] = (v / (1.0 + jnp.exp(-v))).astype(BF16)

    out_ref[...] = product(act_ref[...], own_ref, other_ref)


def mix_attn_kernel(meta_ref, x_ref, part_ref, own_ref, other_ref, out_ref):
    rows = jnp.concatenate(by_core(x_ref, meta_ref), axis=-1)
    out_ref[...] = (part_ref[...] + product(rows, own_ref, other_ref)).astype(BF16)


def mix(kernel, core, x, extras, weights, which, out_dtype, cols, scratch=()):
    sources, rows, _ = x.shape
    groups, half, height, _ = weights[0].shape
    block = pl.BlockSpec((rows, cols * LANES), lambda n: (0, n))
    if which == 0:
        place = height // EDGE - 1
        extra_spec = pl.BlockSpec((None, half, EDGE, LANES), lambda n: (0, 0, place, 0))
    else:
        extra_spec = block
    return pl.pallas_call(
        kernel,
        grid=(groups // cols,),
        in_specs=[
            pl.BlockSpec(memory_space=pltpu.SMEM),
            pl.BlockSpec(x.shape, lambda n: (0, 0, 0)),
        ]
        + [extra_spec] * len(extras)
        + [pl.BlockSpec((cols, half, LANES, LANES), lambda n: (n, 0, which, 0))] * 2,
        out_specs=block,
        out_shape=pltpu.HBM((rows, groups * LANES), out_dtype),
        scratch_shapes=list(scratch),
        compiler_params=params("arbitrary", mb=32),
        cost_estimate=pl.CostEstimate(
            flops=2 * rows * sources * LANES * groups * LANES,
            transcendentals=0,
            bytes_accessed=2 * weights[0].size,
        ),
    )(core, x, *extras, *weights)


def pack_kernel(
    value_ref, gate_ref, query_ref, key_ref, kv_ref, conv_ref, attn_ref, gain_ref, out_ref, in_ref
):
    out_ref[0:LANES, :] = conv_ref[...]
    out_ref[LANES : 2 * LANES, :] = attn_ref[...]
    out_ref[2 * LANES :, :] = jnp.broadcast_to(gain_ref[...].astype(F32), (EDGE, LANES)).astype(BF16)
    both = jnp.concatenate([key_ref[...], kv_ref[...]], 0).astype(F32).T.astype(BF16)
    piece = jnp.concatenate([value_ref[...], gate_ref[...], query_ref[...], both], axis=1)
    for copy in range(in_ref.shape[0]):
        in_ref[copy] = piece


def pack(value, gate, query, key, kv, conv, attn, gain, copies):
    rows = value.shape[0]
    cols = 3 * LANES + 2 * key.shape[1]
    operands = (value, gate, query, key.T, kv.T, conv, attn, gain.reshape(1, LANES))
    shapes = ((2 * LANES + EDGE, LANES), (copies, rows, cols))
    return pl.pallas_call(
        pack_kernel,
        grid=(1,),
        in_specs=[pl.BlockSpec(a.shape, lambda i: (0, 0)) for a in operands],
        out_specs=[
            pl.BlockSpec(shapes[0], lambda i: (0, 0)),
            pl.BlockSpec(shapes[1], lambda i: (0, 0, 0)),
        ],
        out_shape=[
            jax.ShapeDtypeStruct(shapes[0], BF16),
            jax.ShapeDtypeStruct(shapes[1], BF16),
        ],
        compiler_params=pltpu.CompilerParams(vmem_limit_bytes=16 * 1024 * 1024),
        name="pack",
    )(*(in_hbm(a) for a in operands))


def turn_tables(tok_count):
    half = HEAD_DIM // 2
    offset = lax.axis_index("sp") * tok_count
    positions = (offset + jnp.arange(tok_count, dtype=jnp.int32)).astype(F32)
    lane = jnp.arange(LANES, dtype=jnp.int32)
    inverse = ROPE_BASE ** (-(lane % half).astype(F32) / half)
    angles = positions[:, None] * inverse[None, :]
    sign = jnp.where(lane % HEAD_DIM < half, -1.0, 1.0).astype(F32)[None, :]
    return jnp.cos(angles), jnp.sin(angles) * sign


def on_device(
    tokens,
    norm_gain,
    conv_value_weight,
    conv_gate_weight,
    query_weight,
    key_weight,
    value_weight,
    conv_taps,
    conv_gain,
    sink_logit,
    out_conv_weight,
    out_attn_weight,
):
    seqs, length, width = tokens.shape
    sp, tp = lax.axis_size("sp"), lax.axis_size("tp")
    place = jnp.stack([lax.axis_index("sp"), jnp.int32(sp)]).astype(jnp.int32)
    up = [(i, i + 1) for i in range(sp - 1)]
    down = [(i + 1, i) for i in range(sp - 1)]

    out_piece, in_piece = pack(
        conv_value_weight, conv_gate_weight, query_weight, key_weight, value_weight,
        out_conv_weight, out_attn_weight, conv_gain, sp,
    )
    in_weight = lax.all_to_all(in_piece, "sp", 0, 0, tiled=True)
    pieces = [out_piece]
    for d in range(1, tp // 2):
        ring = [(i, (i + 2 * d) % tp) for i in range(tp)]
        pieces.append(lax.ppermute(out_piece, "tp", ring))
    own_weight = lax.all_gather(jnp.concatenate(pieces, axis=0), "sp", axis=0, tiled=True)

    before = lax.ppermute(tokens[:, -EDGE:], "sp", up)
    after = lax.ppermute(tokens[:, :EDGE], "sp", down)
    normed = norm_tokens(tokens.reshape(seqs * length, width), norm_gain)
    cosine, sine = turn_tables(length)
    filtered, query, kv, low, high = project(
        normed, before, after, norm_gain, in_weight, conv_taps, cosine, sine, tp
    )

    before = lax.ppermute(high, "sp", up)
    after = lax.ppermute(low, "sp", down)
    conv_tok = lax.all_to_all(filtered, "tp", 0, 0, tiled=True)
    attn, log_total = attend_inner(sink_logit, query, kv, tp)
    attn, log_total = attend_edge(
        place, sink_logit, query, before, kv, after, attn, log_total
    )
    attn_tok = lax.all_to_all(attn, "tp", 0, 0, tiled=True)

    rows = seqs * length // tp
    own_weight, conv_tok, _ = lax.optimization_barrier((own_weight, conv_tok, log_total))
    other_weight = lax.ppermute(own_weight, "tp", [(i, i ^ 1) for i in range(tp)])
    weights = [
        in_hbm(w.reshape(sp, tp // 2, out_piece.shape[0], LANES))
        for w in (own_weight, other_weight)
    ]
    col = lax.axis_index("tp")
    core = jnp.stack([col % 2, col // 2]).astype(jnp.int32)
    part = mix(
        mix_conv_kernel, core, conv_tok.reshape(tp, rows, LANES), weights, weights, 0, F32, 4,
        [pltpu.VMEM((rows, tp * LANES), BF16)],
    )
    mixed = mix(
        mix_attn_kernel, core, attn_tok.reshape(tp, rows, LANES), [in_hbm(part)], weights, 1, BF16,
        4,
    )
    return mixed.reshape(seqs, length // tp, width), log_total


def solution(mesh):
    placed = (
        P(None, "sp", None),
        P(),
        P("sp", "tp"),
        P("sp", "tp"),
        P("sp", "tp"),
        P("sp", "tp"),
        P("sp", "tp"),
        P(None, "tp"),
        P("tp"),
        P("tp"),
        P("tp", "sp"),
        P("tp", "sp"),
    )

    return jax.shard_map(
        on_device,
        mesh=mesh,
        in_specs=placed,
        out_specs=(P(None, ("sp", "tp"), None), P(None, "tp", "sp")),
        check_vma=False,
    )
```

```python
import functools

import jax
import jax.numpy as jnp
from jax import lax
from jax.experimental import pallas as pl
from jax.experimental.pallas import tpu as pltpu
from jax.sharding import PartitionSpec as P

HEAD_DIM = 64
WINDOW = 128
EPSILON = 1e-06
ROPE_BASE = 10000.0
MASK_VALUE = -1e30
LANES = 128
EDGE = 16
Q_BLOCK = 128
SPAN = Q_BLOCK + 2 * WINDOW
BF16 = jnp.bfloat16
F32 = jnp.float32


def in_hbm(value):
    return pltpu.with_memory_space_constraint(value, pltpu.HBM)


def params(*semantics, mb=48):
    return pltpu.CompilerParams(
        dimension_semantics=semantics, vmem_limit_bytes=mb * 1024 * 1024
    )


def normalize(x, gain):
    x = x.astype(F32)
    mean = jnp.mean(x, axis=-1, keepdims=True)
    centred = x - mean
    variance = jnp.mean(centred * centred, axis=-1, keepdims=True)
    return centred * lax.rsqrt(variance + EPSILON) * gain.astype(F32)


def norm_kernel(x_ref, gain_ref, out_ref):
    out_ref[...] = normalize(x_ref[...], gain_ref[...]).astype(BF16)


def norm_tokens(x, gain, block=512):
    rows, width = x.shape
    block = min(block, rows)
    return pl.pallas_call(
        norm_kernel,
        grid=(rows // block,),
        in_specs=[
            pl.BlockSpec((block, width), lambda i: (i, 0)),
            pl.BlockSpec((1, width), lambda i: (0, 0)),
        ],
        out_specs=pl.BlockSpec((block, width), lambda i: (i, 0)),
        out_shape=pltpu.HBM((rows, width), BF16),
        compiler_params=params("arbitrary", mb=28),
        cost_estimate=pl.CostEstimate(
            flops=40 * rows * width, transcendentals=rows, bytes_accessed=4 * rows * width
        ),
        name="norm_tokens",
    )(in_hbm(x), gain.reshape(1, width))


def project_kernel(
    x_ref, before_ref, after_ref, gain_ref, w_ref, taps_ref, cos_ref, sin_ref, out_ref, q_ref, kv_ref,
    low_ref, high_ref, buf_ref, *, sub, chunk
):
    step = pl.program_id(0)
    dests, _, share, _ = out_ref.shape
    length, seqs = dests * share, before_ref.shape[0]
    half = HEAD_DIM // 2
    tap_count = taps_ref.shape[0]
    shift = EDGE - tap_count // 2
    slot, last = step % 2, (step + 1) % 2
    taps = taps_ref[...].astype(F32)

    def gate(raw):
        return raw[:, :LANES] * jax.nn.sigmoid(raw[:, LANES : 2 * LANES])

    def filter_rows(first):
        for at in range(first, first + sub, chunk):
            total = jnp.zeros((chunk, LANES), F32)
            for tap in range(tap_count):
                rows = buf_ref[last, at + shift + tap : at + shift + tap + chunk, :]
                total = total + rows * taps[tap : tap + 1, :]
            out_ref[at // share, 0, at % share : at % share + chunk, :] = total.astype(BF16)

    @pl.when(step < seqs)
    def _():
        weight = w_ref[...].reshape(-1, w_ref.shape[2])
        lane = lax.broadcasted_iota(jnp.int32, (sub, LANES), 1)
        low, keyed = (lane % HEAD_DIM) < half, lane < HEAD_DIM
        edges = jnp.concatenate([before_ref[step], after_ref[step]], axis=0)
        edges = normalize(edges, gain_ref[...]).astype(BF16)
        ends = gate(
            jnp.dot(edges, weight[:, : 2 * LANES], preferred_element_type=F32)
        ).astype(BF16).astype(F32)
        buf_ref[slot, 0:EDGE, :] = ends[:EDGE]
        buf_ref[slot, EDGE + length : 2 * EDGE + length, :] = ends[EDGE:]
        for first in range(0, length, sub):
            raw = jnp.dot(x_ref[first : first + sub, :], weight, preferred_element_type=F32)
            filter_rows(first)
            buf_ref[slot, EDGE + first : EDGE + first + sub, :] = (
                gate(raw).astype(BF16).astype(F32)
            )
            table = slice(first, first + sub)
            for part, ref, scale in ((2, q_ref, HEAD_DIM**-0.5), (3, kv_ref, None)):
                x = raw[:, part * LANES : (part + 1) * LANES]
                partner = jnp.where(low, pltpu.roll(x, LANES - half, 1), pltpu.roll(x, half, 1))
                cosine, sine = cos_ref[table, :], sin_ref[table, :]
                if part == 3:
                    cosine, sine = jnp.where(keyed, cosine, 1.0), jnp.where(keyed, sine, 0.0)
                turned = x * cosine + partner * sine
                if scale is not None:
                    turned = turned * scale
                turned = turned.astype(BF16)
                ref[0, table, :] = turned
                if part == 3 and first == 0:
                    low_ref[step] = turned[:WINDOW]
                if part == 3 and first + sub == length:
                    high_ref[step] = turned[sub - WINDOW :]

    @pl.when(step == seqs)
    def _():
        for first in range(0, length, sub):
            filter_rows(first)


def project(normed, before, after, gain, weight, taps, cosine, sine, dests, sub=256, chunk=32):
    seqs = before.shape[0]
    rows, width = normed.shape
    length = rows // seqs
    inside = pl.BlockSpec(memory_space=pltpu.VMEM)
    heads = pltpu.HBM((seqs, length, LANES), BF16)
    head_block = pl.BlockSpec((1, length, LANES), lambda s: (jnp.minimum(s, seqs - 1), 0, 0))
    edge_block = pl.BlockSpec((seqs, WINDOW, LANES), lambda s: (0, 0, 0))
    return pl.pallas_call(
        functools.partial(project_kernel, sub=sub, chunk=chunk),
        grid=(seqs + 1,),
        in_specs=[pl.BlockSpec((length, width), lambda s: (jnp.minimum(s, seqs - 1), 0))]
        + [inside] * 4
        + [pl.BlockSpec(taps.shape, lambda s: (0, 0)), inside, inside],
        out_specs=[
            pl.BlockSpec(
                (dests, 1, length // dests, LANES), lambda s: (0, jnp.maximum(s - 1, 0), 0, 0)
            ),
            head_block,
            head_block,
            edge_block,
            edge_block,
        ],
        out_shape=[
            jax.ShapeDtypeStruct((dests, seqs, length // dests, LANES), BF16), heads, heads
        ]
        + [pltpu.HBM((seqs, WINDOW, LANES), BF16)] * 2,
        scratch_shapes=[pltpu.VMEM((2, length + 2 * EDGE, LANES), F32)],
        compiler_params=params("arbitrary", mb=28),
        cost_estimate=pl.CostEstimate(
            flops=2 * rows * width * weight.shape[2],
            transcendentals=0,
            bytes_accessed=2 * rows * width,
        ),
        name="project",
    )(in_hbm(normed), before, after, gain.reshape(1, width), weight, in_hbm(taps), cosine, sine)


def band_bias(first, last):
    query = lax.broadcasted_iota(jnp.int32, (Q_BLOCK, SPAN), 0)
    key = lax.broadcasted_iota(jnp.int32, (Q_BLOCK, SPAN), 1)
    allowed = (key >= query) & (key <= query + 2 * WINDOW) & (key >= first) & (key < last)
    return jnp.where(allowed, 0.0, MASK_VALUE).astype(F32)


def attend_blocks(sink_ref, jobs):
    low = lax.broadcasted_iota(jnp.int32, (Q_BLOCK, LANES), 1) < HEAD_DIM
    low_both = lax.broadcasted_iota(jnp.int32, (2 * Q_BLOCK, LANES), 1) < HEAD_DIM
    diagonal = lax.broadcasted_iota(jnp.int32, (LANES, LANES), 0) == lax.broadcasted_iota(
        jnp.int32, (LANES, LANES), 1
    )
    is_first = lax.broadcasted_iota(jnp.int32, (2 * Q_BLOCK, 1), 0) < Q_BLOCK
    sink = jnp.where(is_first, sink_ref[0], sink_ref[1])

    def score(job):
        query, bias = job[0](), job[3]()
        swapped = pltpu.roll(query.astype(F32), HEAD_DIM, 1).astype(BF16)
        own = jnp.concatenate([query, swapped], 0)
        own = jnp.where(low_both, own, jnp.zeros_like(own))
        scores = lax.dot_general(
            own, job[1](), (((1,), (1,)), ((), ())), preferred_element_type=F32
        )
        return scores + jnp.concatenate([bias, bias], 0)

    def weigh(scores):
        top = jnp.maximum(jnp.max(scores, axis=-1, keepdims=True), sink)
        return top, jnp.exp(scores - top).astype(BF16)

    def blend(job, top, weights):
        both = jnp.dot(weights, job[2](), preferred_element_type=F32)
        swapped = pltpu.roll(both, HEAD_DIM, 1)
        total = jnp.where(low_both, both, swapped) + jnp.exp(sink - top)
        log_total = top + jnp.log(total)
        logs = [
            jnp.sum(
                jnp.where(diagonal, log_total[head * Q_BLOCK : (head + 1) * Q_BLOCK], 0.0),
                axis=0,
                keepdims=True,
            )
            for head in range(2)
        ]
        first = swapped[:Q_BLOCK] / total[:Q_BLOCK]
        second = both[Q_BLOCK:] / total[Q_BLOCK:]
        job[4](jnp.where(low, first, second).astype(BF16), logs)

    ahead, behind = score(jobs[0]), None
    for at, job in enumerate(jobs):
        scores = ahead
        if at + 1 < len(jobs):
            ahead = score(jobs[at + 1])
        top, weights = weigh(scores)
        if behind is not None:
            blend(jobs[at - 1], *behind)
        behind = top, weights
    blend(jobs[-1], *behind)


def with_ones(keys):
    in_low = lax.broadcasted_iota(jnp.int32, keys.shape, keys.ndim - 1) < HEAD_DIM
    return jnp.where(in_low, jnp.ones_like(keys), keys)


def inner_kernel(sink_ref, q_ref, kv_ref, out_ref, log_ref, one_ref, bias_ref):
    length = kv_ref.shape[1]

    @pl.when(pl.program_id(0) == 0)
    def _():
        bias_ref[...] = band_bias(0, SPAN)

    one_ref[...] = with_ones(kv_ref[0])

    def job(block):
        at = block * Q_BLOCK
        span = slice(at - WINDOW, at + Q_BLOCK + WINDOW)

        def store(out, logs):
            out_ref[block, 0] = out
            for head in range(2):
                log_ref[0, head : head + 1, at : at + Q_BLOCK] = logs[head]

        return (
            lambda: q_ref[0, at : at + Q_BLOCK, :],
            lambda: kv_ref[0, span, :],
            lambda: one_ref[span, :],
            lambda: bias_ref[...],
            store,
        )

    attend_blocks(sink_ref, [job(block) for block in range(1, length // Q_BLOCK - 1)])


def attend_inner(sink, query, kv, dests):
    seqs, length, _ = kv.shape
    whole = pl.BlockSpec((1, length, LANES), lambda s: (s, 0, 0))
    return pl.pallas_call(
        inner_kernel,
        grid=(seqs,),
        in_specs=[pl.BlockSpec(memory_space=pltpu.SMEM), whole, whole],
        out_specs=[
            pl.BlockSpec((dests, 1, length // dests, LANES), lambda s: (0, s, 0, 0)),
            pl.BlockSpec((1, 2, length), lambda s: (s, 0, 0)),
        ],
        out_shape=[
            pltpu.HBM((dests, seqs, length // dests, LANES), BF16),
            pltpu.HBM((seqs, 2, length), F32),
        ],
        scratch_shapes=[
            pltpu.VMEM((length, LANES), BF16),
            pltpu.VMEM((Q_BLOCK, SPAN), F32),
        ],
        compiler_params=params("arbitrary", mb=28),
        cost_estimate=pl.CostEstimate(
            flops=40 * seqs * length * SPAN * LANES // 8,
            transcendentals=0,
            bytes_accessed=6 * seqs * length * LANES,
        ),
        name="attend_inner",
    )(sink, in_hbm(query), in_hbm(kv))


def edge_kernel(
    place_ref, sink_ref, q_low_ref, q_high_ref, before_ref, kv_low_ref, kv_high_ref, after_ref,
    _, __, out_ref, log_ref, pad_ref, one_ref, bias_ref, own_ref, own_log_ref, sems
):
    seqs = before_ref.shape[0]
    blocks = out_ref.shape[0]
    bias_ref[0] = band_bias(jnp.where(place_ref[0] == 0, WINDOW, 0), SPAN)
    bias_ref[1] = band_bias(
        0, jnp.where(place_ref[0] == place_ref[1] - 1, Q_BLOCK + WINDOW, SPAN)
    )
    pad_ref[0, :, :WINDOW] = before_ref[...]
    pad_ref[0, :, WINDOW:] = kv_low_ref[...]
    pad_ref[1, :, : SPAN - WINDOW] = kv_high_ref[...]
    pad_ref[1, :, SPAN - WINDOW :] = after_ref[...]
    one_ref[...] = with_ones(pad_ref[...])

    def job(side, seq):
        def store(out, logs):
            own_ref[side, seq] = out
            for head in range(2):
                own_log_ref[side, seq, head : head + 1, :] = logs[head]

        return (
            lambda: (q_low_ref, q_high_ref)[side][seq],
            lambda: pad_ref[side, seq],
            lambda: one_ref[side, seq],
            lambda: bias_ref[side],
            store,
        )

    attend_blocks(sink_ref, [job(side, seq) for side in range(2) for seq in range(seqs)])
    copies = []
    for side, block in enumerate((0, blocks - 1)):
        copies.append(
            pltpu.make_async_copy(own_ref.at[side], out_ref.at[block], sems.at[side, 0])
        )
        copies.append(
            pltpu.make_async_copy(
                own_log_ref.at[side],
                log_ref.at[:, :, pl.ds(block * Q_BLOCK, Q_BLOCK)],
                sems.at[side, 1],
            )
        )
    for copy in copies:
        copy.start()
    for copy in copies:
        copy.wait()


def attend_edge(place, sink, query, before, kv, after, out, log_total):
    seqs, length, _ = kv.shape
    ends = SPAN - WINDOW
    smem = pl.BlockSpec(memory_space=pltpu.SMEM)
    raw = pl.BlockSpec(memory_space=pl.ANY)

    def rows(count, at):
        return pl.BlockSpec((seqs, count, LANES), lambda i: (0, at, 0))

    return pl.pallas_call(
        edge_kernel,
        grid=(1,),
        in_specs=[
            smem,
            smem,
            rows(Q_BLOCK, 0),
            rows(Q_BLOCK, length // Q_BLOCK - 1),
            rows(WINDOW, 0),
            rows(ends, 0),
            rows(ends, length // ends - 1),
            rows(WINDOW, 0),
            raw,
            raw,
        ],
        out_specs=[raw, raw],
        out_shape=[pltpu.HBM(out.shape, BF16), pltpu.HBM(log_total.shape, F32)],
        input_output_aliases={8: 0, 9: 1},
        scratch_shapes=[
            pltpu.VMEM((2, seqs, SPAN, LANES), BF16),
            pltpu.VMEM((2, seqs, SPAN, LANES), BF16),
            pltpu.VMEM((2, Q_BLOCK, SPAN), F32),
            pltpu.VMEM((2, seqs, Q_BLOCK, LANES), BF16),
            pltpu.VMEM((2, seqs, 2, Q_BLOCK), F32),
            pltpu.SemaphoreType.DMA((2, 2)),
        ],
        compiler_params=params("arbitrary", mb=28),
        cost_estimate=pl.CostEstimate(
            flops=10 * seqs * length * SPAN * LANES // 8,
            transcendentals=0,
            bytes_accessed=2 * seqs * length * LANES,
        ),
        name="attend_edge",
    )(place, sink, in_hbm(query), in_hbm(query), before, in_hbm(kv), in_hbm(kv), after,
      in_hbm(out), in_hbm(log_total))


def side_by_side(ref):
    return jnp.concatenate([ref[i] for i in range(ref.shape[0])], axis=-1)


def by_core(ref, meta_ref):
    core, y = meta_ref[0], meta_ref[1]
    count = ref.shape[0] // 2
    places = [2 * ((y - step + count) % count) for step in range(count)]
    own = [ref[place + core] for place in places]
    other = [ref[place + 1 - core] for place in places]
    return jnp.concatenate(own, axis=-1), jnp.concatenate(other, axis=-1)


def columns(ref):
    return jnp.concatenate([ref[c].reshape(-1, LANES) for c in range(ref.shape[0])], axis=-1)


def product(rows, own_ref, other_ref):
    both = jnp.concatenate([columns(own_ref), columns(other_ref)], axis=0)
    return jnp.dot(rows, both, preferred_element_type=F32)


def mix_conv_kernel(
    meta_ref, x_ref, own_gain_ref, other_gain_ref, own_ref, other_ref, out_ref, act_ref
):
    @pl.when(pl.program_id(0) == 0)
    def _():
        x = jnp.concatenate(by_core(x_ref, meta_ref), axis=-1)
        gain = jnp.concatenate([side_by_side(own_gain_ref), side_by_side(other_gain_ref)], axis=-1)
        v = normalize(x, gain[0:1])
        act_ref[...] = (v / (1.0 + jnp.exp(-v))).astype(BF16)

    out_ref[...] = product(act_ref[...], own_ref, other_ref)


def mix_attn_kernel(meta_ref, x_ref, part_ref, own_ref, other_ref, out_ref):
    rows = jnp.concatenate(by_core(x_ref, meta_ref), axis=-1)
    out_ref[...] = (part_ref[...] + product(rows, own_ref, other_ref)).astype(BF16)


def mix(kernel, core, x, extras, weights, which, out_dtype, cols, scratch=()):
    sources, rows, _ = x.shape
    groups, half, height, _ = weights[0].shape
    block = pl.BlockSpec((rows, cols * LANES), lambda n: (0, n))
    if which == 0:
        place = height // EDGE - 1
        extra_spec = pl.BlockSpec((None, half, EDGE, LANES), lambda n: (0, 0, place, 0))
    else:
        extra_spec = block
    return pl.pallas_call(
        kernel,
        grid=(groups // cols,),
        in_specs=[
            pl.BlockSpec(memory_space=pltpu.SMEM),
            pl.BlockSpec(x.shape, lambda n: (0, 0, 0)),
        ]
        + [extra_spec] * len(extras)
        + [pl.BlockSpec((cols, half, LANES, LANES), lambda n: (n, 0, which, 0))] * 2,
        out_specs=block,
        out_shape=pltpu.HBM((rows, groups * LANES), out_dtype),
        scratch_shapes=list(scratch),
        compiler_params=params("arbitrary", mb=32),
        cost_estimate=pl.CostEstimate(
            flops=2 * rows * sources * LANES * groups * LANES,
            transcendentals=0,
            bytes_accessed=2 * weights[0].size,
        ),
    )(core, x, *extras, *weights)


def pack_kernel(
    value_ref, gate_ref, query_ref, key_ref, kv_ref, conv_ref, attn_ref, gain_ref, out_ref, in_ref
):
    out_ref[0:LANES, :] = conv_ref[...]
    out_ref[LANES : 2 * LANES, :] = attn_ref[...]
    out_ref[2 * LANES :, :] = jnp.broadcast_to(gain_ref[...].astype(F32), (EDGE, LANES)).astype(BF16)
    both = jnp.concatenate([key_ref[...], kv_ref[...]], 0).astype(F32).T.astype(BF16)
    piece = jnp.concatenate([value_ref[...], gate_ref[...], query_ref[...], both], axis=1)
    for copy in range(in_ref.shape[0]):
        in_ref[copy] = piece


def pack(value, gate, query, key, kv, conv, attn, gain, copies):
    rows = value.shape[0]
    cols = 3 * LANES + 2 * key.shape[1]
    operands = (value, gate, query, key.T, kv.T, conv, attn, gain.reshape(1, LANES))
    shapes = ((2 * LANES + EDGE, LANES), (copies, rows, cols))
    return pl.pallas_call(
        pack_kernel,
        grid=(1,),
        in_specs=[pl.BlockSpec(a.shape, lambda i: (0, 0)) for a in operands],
        out_specs=[
            pl.BlockSpec(shapes[0], lambda i: (0, 0)),
            pl.BlockSpec(shapes[1], lambda i: (0, 0, 0)),
        ],
        out_shape=[
            jax.ShapeDtypeStruct(shapes[0], BF16),
            jax.ShapeDtypeStruct(shapes[1], BF16),
        ],
        compiler_params=pltpu.CompilerParams(vmem_limit_bytes=16 * 1024 * 1024),
        name="pack",
    )(*(in_hbm(a) for a in operands))


def turn_tables(tok_count):
    half = HEAD_DIM // 2
    offset = lax.axis_index("sp") * tok_count
    positions = (offset + jnp.arange(tok_count, dtype=jnp.int32)).astype(F32)
    lane = jnp.arange(LANES, dtype=jnp.int32)
    inverse = ROPE_BASE ** (-(lane % half).astype(F32) / half)
    angles = positions[:, None] * inverse[None, :]
    sign = jnp.where(lane % HEAD_DIM < half, -1.0, 1.0).astype(F32)[None, :]
    return jnp.cos(angles), jnp.sin(angles) * sign


def on_device(
    tokens,
    norm_gain,
    conv_value_weight,
    conv_gate_weight,
    query_weight,
    key_weight,
    value_weight,
    conv_taps,
    conv_gain,
    sink_logit,
    out_conv_weight,
    out_attn_weight,
):
    seqs, length, width = tokens.shape
    sp, tp = lax.axis_size("sp"), lax.axis_size("tp")
    place = jnp.stack([lax.axis_index("sp"), jnp.int32(sp)]).astype(jnp.int32)
    up = [(i, i + 1) for i in range(sp - 1)]
    down = [(i + 1, i) for i in range(sp - 1)]

    out_piece, in_piece = pack(
        conv_value_weight, conv_gate_weight, query_weight, key_weight, value_weight,
        out_conv_weight, out_attn_weight, conv_gain, sp,
    )
    in_weight = lax.all_to_all(in_piece, "sp", 0, 0, tiled=True)
    pieces = [out_piece]
    for d in range(1, tp // 2):
        ring = [(i, (i + 2 * d) % tp) for i in range(tp)]
        pieces.append(lax.ppermute(out_piece, "tp", ring))
    own_weight = lax.all_gather(jnp.concatenate(pieces, axis=0), "sp", axis=0, tiled=True)

    before = lax.ppermute(tokens[:, -EDGE:], "sp", up)
    after = lax.ppermute(tokens[:, :EDGE], "sp", down)
    normed = norm_tokens(tokens.reshape(seqs * length, width), norm_gain)
    cosine, sine = turn_tables(length)
    filtered, query, kv, low, high = project(
        normed, before, after, norm_gain, in_weight, conv_taps, cosine, sine, tp
    )

    before = lax.ppermute(high, "sp", up)
    after = lax.ppermute(low, "sp", down)
    conv_tok = lax.all_to_all(filtered, "tp", 0, 0, tiled=True)
    attn, log_total = attend_inner(sink_logit, query, kv, tp)
    attn, log_total = attend_edge(
        place, sink_logit, query, before, kv, after, attn, log_total
    )
    attn_tok = lax.all_to_all(attn, "tp", 0, 0, tiled=True)

    rows = seqs * length // tp
    own_weight, conv_tok, _ = lax.optimization_barrier((own_weight, conv_tok, log_total))
    other_weight = lax.ppermute(own_weight, "tp", [(i, i ^ 1) for i in range(tp)])
    weights = [
        in_hbm(w.reshape(sp, tp // 2, out_piece.shape[0], LANES))
        for w in (own_weight, other_weight)
    ]
    col = lax.axis_index("tp")
    core = jnp.stack([col % 2, col // 2]).astype(jnp.int32)
    part = mix(
        mix_conv_kernel, core, conv_tok.reshape(tp, rows, LANES), weights, weights, 0, F32, 4,
        [pltpu.VMEM((rows, tp * LANES), BF16)],
    )
    mixed = mix(
        mix_attn_kernel, core, attn_tok.reshape(tp, rows, LANES), [in_hbm(part)], weights, 1, BF16,
        4,
    )
    return mixed.reshape(seqs, length // tp, width), log_total


def solution(mesh):
    placed = (
        P(None, "sp", None),
        P(),
        P("sp", "tp"),
        P("sp", "tp"),
        P("sp", "tp"),
        P("sp", "tp"),
        P("sp", "tp"),
        P(None, "tp"),
        P("tp"),
        P("tp"),
        P("tp", "sp"),
        P("tp", "sp"),
    )

    return jax.shard_map(
        on_device,
        mesh=mesh,
        in_specs=placed,
        out_specs=(P(None, ("sp", "tp"), None), P(None, "tp", "sp")),
        check_vma=False,
    )
```
